128 devices in a mesh: rep: 2 (over z_hi), fs: 32 (over z_lo, y, x), tp: 2 (over core).
Axes of the slice: x: 4, y: 4, z: 4 (z_hi: 2, z_lo: 2; z = z_hi * 2 + z_lo), core: 2. Of those that a mesh axis runs over, the one named last changes fastest.
Arguments:
- resid: bfloat16 [65536, 2048], P(('rep', 'fs'), 'tp'), may hold values from -6 to 6
- gain_mix_in: float32 [2048], replicated, may hold values from 0.1 to 1.9
- u_weight: float32 [2048, 1024], P('fs', 'tp'), may hold values from -0.125 to 0.125
- v_weight: float32 [2048, 1024], P('fs', 'tp'), may hold values from -0.125 to 0.125
- u_scale: float32 [1024], P('tp'), may hold values from 0.5 to 2
- v_scale: float32 [1024], P('tp'), may hold values from 0.3 to 3
- v_gain: float32 [1024], P('tp'), may hold values from 0.1 to 1.9
- mix_matrix: float32 [16, 128, 128], P('tp'), may hold values from -0.5 to 0.5
- mix_bias: float32 [16, 128], P('tp'), may hold values from 0.1 to 1.9
- out_weight: float32 [1024, 2048], P('tp', 'fs'), may hold values from -0.1875 to 0.1875
- out_scale: float32 [2048], P('fs'), may hold values from 0.3 to 3
- gain_mix_out: float32 [2048], replicated, may hold values from 0.1 to 1.9
- gain_ffn_in: float32 [2048], replicated, may hold values from 0.1 to 1.9
- up_weight: float32 [2048, 4096], P('fs', 'tp'), may hold values from -0.125 to 0.125
- up_scale: float32 [4096], P('tp'), may hold values from 0.5 to 2
- down_weight: float32 [4096, 2048], P('tp', 'fs'), may hold values from -0.09375 to 0.09375
- down_scale: float32 [2048], P('fs'), may hold values from 0.3 to 3
- gain_ffn_out: float32 [2048], replicated, may hold values from 0.1 to 1.9
Outputs:
- result: bfloat16 [65536, 2048], P(('rep', 'fs'), 'tp')
The draws below stay inside these ranges and needn't reach their ends.
All inputs are finite; a program needn't handle non-finite values.
Results may differ from the reference program's by a relative error of at most 0.013.
Values may be sent and summed in bfloat16 or wider, within the bound.
A program may use at most 128 MiB of HBM per device.

```python
import math
import jax
import jax.numpy as jnp
from jax import lax

D = 2048
A = 1024
GROUPS = 16
FF = 4096
BLOCK = 128
TOKENS = 65536
N_TP = 2


def shard_levels(key, dims, split, smallest, high):
    loudness = 1.0
    for dim, shards_of in split:
        heights = jax.random.uniform(jax.random.fold_in(jax.random.fold_in(key, 6), dim), (shards_of,), jnp.float32, smallest / len(split), high / len(split))
        loudness = loudness * jnp.repeat(jnp.exp(heights), dims[dim] // shards_of).reshape((-1,) + (1,) * (len(dims) - 1 - dim))
    return loudness


def normal_values(own_key, dims, scale, bound, shards=(), kind=jnp.bfloat16):
    loudness = shard_levels(own_key, dims, shards, -0.22, 0.18) if shards else 1.0
    drawn = jax.random.normal(own_key, dims, jnp.float32) * scale * loudness
    return jnp.minimum(jnp.maximum(drawn, -bound), bound).astype(kind)


def setup_inputs(seed: int = 0) -> dict:
    streams_of = jax.random.split(jax.random.key(seed), 19)
    return {
        "resid": normal_values(streams_of[0], (TOKENS, D), 1.0, 6.0, ((0, 64), (1, 2))),
        "gain_mix_in": jnp.clip(1.0 + 0.18 * jax.random.normal(streams_of[1], (D,), jnp.float32), 0.1, 1.9),
        "u_weight": normal_values(streams_of[2], (D, A), D ** -0.5, 0.125, ((0, 32), (1, 2)), jnp.float32),
        "v_weight": normal_values(streams_of[3], (D, A), D ** -0.5, 0.125, ((0, 32), (1, 2)), jnp.float32),
        "u_scale": jnp.clip(jnp.exp(math.log(2.0) - 1.3862944 * jax.random.uniform(streams_of[4], (A,), jnp.float32) ** shard_levels(streams_of[4], (A,), ((0, 2),), -0.2, 0.2)), 0.5, 2.0),
        "v_scale": jnp.clip(jnp.exp(math.log(3.0) - 2.3025851 * jax.random.uniform(streams_of[5], (A,), jnp.float32) ** shard_levels(streams_of[5], (A,), ((0, 2),), -0.2, 0.2)), 0.3, 3.0),
        "v_gain": jnp.clip(1.0 + 0.18 * jax.random.normal(streams_of[6], (A,), jnp.float32), 0.1, 1.9),
        "mix_matrix": normal_values(streams_of[7], (GROUPS, BLOCK, BLOCK), BLOCK ** -0.5, 0.5, ((0, 2),), jnp.float32),
        "mix_bias": jnp.clip(1.0 + 0.18 * jax.random.normal(streams_of[8], (GROUPS, BLOCK), jnp.float32), 0.1, 1.9),
        "out_weight": normal_values(streams_of[9], (A, D), A ** -0.5, 0.1875, ((0, 2), (1, 32)), jnp.float32),
        "out_scale": jnp.clip(jnp.exp(math.log(3.0) - 2.3025851 * jax.random.uniform(streams_of[10], (D,), jnp.float32) ** shard_levels(streams_of[10], (D,), ((0, 32),), -0.2, 0.2)), 0.3, 3.0),
        "gain_mix_out": jnp.clip(1.0 + 0.18 * jax.random.normal(streams_of[11], (D,), jnp.float32), 0.1, 1.9),
        "gain_ffn_in": jnp.clip(1.0 + 0.18 * jax.random.normal(streams_of[12], (D,), jnp.float32), 0.1, 1.9),
        "up_weight": normal_values(streams_of[13], (D, FF), D ** -0.5, 0.125, ((0, 32), (1, 2)), jnp.float32),
        "up_scale": jnp.clip(jnp.exp(math.log(2.0) - 1.3862944 * jax.random.uniform(streams_of[14], (FF,), jnp.float32) ** shard_levels(streams_of[14], (FF,), ((0, 2),), -0.2, 0.2)), 0.5, 2.0),
        "down_weight": normal_values(streams_of[15], (FF, D), FF ** -0.5, 0.09375, ((0, 2), (1, 32)), jnp.float32),
        "down_scale": jnp.clip(jnp.exp(math.log(3.0) - 2.3025851 * jax.random.uniform(streams_of[16], (D,), jnp.float32) ** shard_levels(streams_of[16], (D,), ((0, 32),), -0.2, 0.2)), 0.3, 3.0),
        "gain_ffn_out": jnp.clip(1.0 + 0.18 * jax.random.normal(streams_of[17], (D,), jnp.float32), 0.1, 1.9),
    }


def rms_norm(values, gain):
    power = lax.optimization_barrier(jnp.mean(values * values, axis=-1, keepdims=True))
    return values * lax.rsqrt(power + 1e-06) * gain

def split_sum(left, right, pieces):
    width = left.shape[1] // pieces
    total = jnp.zeros((left.shape[0], right.shape[1]), jnp.float32)
    for index in range(pieces):
        lower = index * width
        partial_value = jnp.dot(left[:, lower:lower + width], right[lower:lower + width], preferred_element_type=jnp.float32)
        rounded = lax.optimization_barrier(partial_value.astype(jnp.bfloat16))
        total = total + rounded.astype(jnp.float32)
    return total

def reference(resid, gain_mix_in, u_weight, v_weight, u_scale, v_scale, v_gain, mix_matrix, mix_bias, out_weight, out_scale, gain_mix_out, gain_ffn_in, up_weight, up_scale, down_weight, down_scale, gain_ffn_out):
    stream = resid.astype(jnp.float32)
    normed = rms_norm(stream, gain_mix_in).astype(jnp.bfloat16)
    u_act = jax.nn.gelu(jnp.dot(normed, u_weight.astype(jnp.bfloat16), preferred_element_type=jnp.float32) * u_scale)
    v_act = jax.nn.gelu(jnp.dot(normed, v_weight.astype(jnp.bfloat16), preferred_element_type=jnp.float32) * v_scale)
    centre = lax.optimization_barrier(jnp.mean(v_act, axis=-1, keepdims=True))
    spread = lax.optimization_barrier(jnp.mean(jnp.square(v_act - centre), axis=-1, keepdims=True))
    v_norm = ((v_act - centre) * lax.rsqrt(spread + 1e-06) * v_gain).astype(jnp.bfloat16)
    tokens = resid.shape[0]
    groups = mix_matrix.shape[0]
    blocks = v_norm.reshape(tokens // BLOCK, BLOCK, groups, A // groups).astype(jnp.float32)
    matrix = mix_matrix.astype(jnp.bfloat16).astype(jnp.float32)
    mixed = jnp.einsum('gts,bsgd->btgd', matrix, blocks) + mix_bias.T[None, :, :, None]
    gated = (u_act * mixed.reshape(tokens, A)).astype(jnp.bfloat16)
    mix_out = split_sum(gated, out_weight.astype(jnp.bfloat16), N_TP) * out_scale
    middle = (stream + rms_norm(mix_out, gain_mix_out)).astype(jnp.bfloat16)
    ffn_in = rms_norm(middle.astype(jnp.float32), gain_ffn_in).astype(jnp.bfloat16)
    raised = jnp.dot(ffn_in, up_weight.astype(jnp.bfloat16), preferred_element_type=jnp.float32) * up_scale
    hidden = jnp.square(jax.nn.relu(raised)).astype(jnp.bfloat16)
    ffn_out = split_sum(hidden, down_weight.astype(jnp.bfloat16), N_TP) * down_scale
    return (middle.astype(jnp.float32) + rms_norm(ffn_out, gain_ffn_out)).astype(jnp.bfloat16)
```

```python
import functools

import jax
import jax.numpy as jnp
from jax import lax
from jax.experimental import pallas as pl
from jax.experimental.pallas import tpu as pltpu
from jax.sharding import PartitionSpec as P

MESH = pl.DeviceIdType.MESH
BF = jnp.bfloat16
F32 = jnp.float32

ROWS = 1024
WIDTH = 2048
HALF = 1024
COLS = 512
NCH = 11
STEPS = 5
SHARDS = 32
TILE = 16
GROUPS_OF_ROWS = 4
RB = 256
NRB = ROWS // RB
EB = 32

ORDERS = (
    (
        ("QY", "PY", "O", "QX", "PX"),
        ("QY", "PX", "PY", "QX", "O"),
        ("PX", "QX", "S", "PY", "QY"),
        ("PX", "QY", "QX", "PY", "S"),
    ),
    (
        ("PX", "QX", "QY", "PY", "S"),
        ("QX", "QY", "S", "PY", "PX"),
        ("QY", "PX", "PY", "QX", "O"),
        ("PY", "O", "PX", "QX", "QY"),
    ),
)
SCALE_ORDER = ("PX", "QY", "QX", "PY", "S")


def link_bits(fs):
    x, y, z = fs % 4, (fs // 4) % 4, fs // 16
    return {
        "PX": (x + x // 2) % 2,
        "QX": x // 2,
        "PY": (y + y // 2) % 2,
        "QY": y // 2,
        "S": z,
        "O": z,
    }


def place(order, fs):
    bits = link_bits(fs)
    return sum(bits[name] * (1 << k) for k, name in enumerate(order))


def order_of(c, r):
    return ORDERS[c % 2][r]


def block_rows(c, first, count):
    out = []
    for s in range(first, first + count):
        for r in range(GROUPS_OF_ROWS):
            out.append((r, place(order_of(c, r), s)))
    return out


def gathered_rows(buf, c, first=0, count=SHARDS):
    return jnp.concatenate([buf[c, r, p] for r, p in block_rows(c, first, count)], axis=0)


def dot_nt(a, b):
    return lax.dot_general(a, b, (((1,), (1,)), ((), ())), preferred_element_type=F32)


def kernel(
    pieces,
    resid,
    own_scales,
    gain_in,
    gain_out,
    gain_up,
    gain_last,
    u_scale,
    v_scale,
    v_gain,
    mix_matrix,
    bias,
    up_scale,
    result,
    buf,
    sbuf,
    scales,
    xfull,
    nbuf,
    acc,
    vn,
    gated,
    part,
    part_in,
    mid,
    hid,
    terms,
    terms_in,
    stats,
    stats_in,
    load_sem,
    send_sem,
    recv_sem,
    s_send,
    s_recv,
    x_sem,
    pair_send,
    pair_recv,
    out_sem,
):
    rep, fs, lane = lax.axis_index("rep"), lax.axis_index("fs"), lax.axis_index("tp")
    x, y, z = fs % 4, (fs // 4) % 4, fs // 16
    here = z * 16 + y * 4
    far = (1 - z) * 16 + y * 4 + x
    peer = {
        "PX": (rep, here + x + 1 - 2 * (x % 2), lane),
        "QX": (rep, here + 3 - x, lane),
        "PY": (rep, z * 16 + (y + 1 - 2 * (y % 2)) * 4 + x, lane),
        "QY": (rep, z * 16 + (3 - y) * 4 + x, lane),
        "S": (rep, far, lane),
        "O": (1 - rep, far, lane),
    }
    partner = (rep, fs, 1 - lane)
    places = {o: place(o, fs) for o in set_of_orders()}

    for c in range(NCH):
        for r in range(GROUPS_OF_ROWS):
            pltpu.make_async_copy(
                pieces.at[c, r], buf.at[c, r, places[order_of(c, r)]], load_sem.at[c]
            ).start()
    pltpu.make_async_copy(own_scales, sbuf.at[places[SCALE_ORDER]], load_sem.at[NCH]).start()
    own_x = pltpu.make_async_copy(resid, xfull.at[lane], x_sem.at[0])
    own_x.start()

    barrier = pltpu.get_barrier_semaphore()
    for device in (*peer.values(), partner):
        pl.semaphore_signal(barrier, inc=1, device_id=device, device_id_type=MESH)
    pl.semaphore_wait(barrier, 7)

    other_x = pltpu.make_async_remote_copy(
        src_ref=resid,
        dst_ref=xfull.at[lane],
        send_sem=x_sem.at[1],
        recv_sem=x_sem.at[2],
        device_id=partner,
        device_id_type=MESH,
    )
    other_x.start()

    def send(c, k):
        size = 1 << k
        for r in range(GROUPS_OF_ROWS):
            order = order_of(c, r)
            base = (places[order] // size) * size
            block = buf.at[c, r, pl.ds(base, size)]
            pltpu.make_async_remote_copy(
                src_ref=block,
                dst_ref=block,
                send_sem=send_sem.at[c],
                recv_sem=recv_sem.at[c, k],
                device_id=peer[order[k]],
                device_id_type=MESH,
            ).start()

    def arrived(c, k):
        block = buf.at[c, :, pl.ds(0, 1 << k)]
        pltpu.make_async_copy(block, block, recv_sem.at[c, k]).wait()

    def loaded(c):
        block = buf.at[c, :, 0]
        pltpu.make_async_copy(block, block, load_sem.at[c]).wait()

    def send_scales(k):
        size = 1 << k
        base = (places[SCALE_ORDER] // size) * size
        block = sbuf.at[pl.ds(base, size)]
        pltpu.make_async_remote_copy(
            src_ref=block,
            dst_ref=block,
            send_sem=s_send.at[k],
            recv_sem=s_recv.at[k],
            device_id=peer[SCALE_ORDER[k]],
            device_id_type=MESH,
        ).start()

    def scales_arrived(k):
        block = sbuf.at[pl.ds(0, 1 << k)]
        pltpu.make_async_copy(block, block, s_recv.at[k]).wait()

    def substep(t, k):
        c = t - k
        if 0 <= c < NCH:
            if k == 0:
                loaded(c)
            else:
                arrived(c, k - 1)
            send(c, k)

    def to_partner(src, dst, index):
        return pltpu.make_async_remote_copy(
            src_ref=src,
            dst_ref=dst,
            send_sem=pair_send.at[index],
            recv_sem=pair_recv.at[index],
            device_id=partner,
            device_id_type=MESH,
        )

    def x_normed():
        own_x.wait()
        other_x.wait()
        def body(i, _):
            rows = pl.ds(pl.multiple_of(i * EB, EB), EB)
            a = xfull[0, rows, :].astype(F32)
            b = xfull[1, rows, :].astype(F32)
            power = jnp.sum(a * a, axis=1, keepdims=True) + jnp.sum(b * b, axis=1, keepdims=True)
            inv = lax.rsqrt(power / WIDTH + 1e-06)
            nbuf[rows, :HALF] = (a * inv * gain_in[:, :HALF]).astype(BF)
            nbuf[rows, HALF:] = (b * inv * gain_in[:, HALF:]).astype(BF)
            return 0
        lax.fori_loop(0, ROWS // EB, body, 0)

    def row_block(i):
        return pl.ds(pl.multiple_of(i * RB, RB), RB)

    def u_part(first, last):
        def body(i, _):
            rows = row_block(i)
            w = gathered_rows(buf, 0)
            pre = jnp.dot(nbuf[rows, :], w, preferred_element_type=F32)
            acc[rows, :COLS] = jax.nn.gelu(pre * u_scale[...])
            return 0
        lax.fori_loop(first, last, body, 0)

    def v_part(first, last):
        def body(i, _):
            rows = row_block(i)
            w = gathered_rows(buf, 1)
            pre = jnp.dot(nbuf[rows, :], w, preferred_element_type=F32)
            act = jax.nn.gelu(pre * v_scale[...])
            acc[rows, COLS : 2 * COLS] = act
            total = jnp.sum(act, axis=1, keepdims=True)
            off = act - total / COLS
            spread = jnp.sum(off * off, axis=1, keepdims=True)
            lanes = lax.broadcasted_iota(jnp.int32, (RB, 128), 1)
            stats[0, rows, :] = jnp.where(lanes == 0, total, spread)
            return 0
        lax.fori_loop(first, last, body, 0)

    def v_normed(first, last):
        def body(i, _):
            rows = pl.ds(pl.multiple_of(i * EB, EB), EB)
            act = acc[rows, COLS : 2 * COLS]
            own, other = stats[0, rows, :], stats_in[0, rows, :]
            total = own[:, 0:1] + other[:, 0:1]
            apart = (own[:, 0:1] - other[:, 0:1]) / COLS
            spread = own[:, 1:2] + other[:, 1:2] + apart * apart * (COLS / 2)
            centre = total / (2 * COLS)
            inv = lax.rsqrt(spread / (2 * COLS) + 1e-06)
            vn[rows, :] = ((act - centre) * inv * v_gain[...]).astype(BF)
            return 0
        lax.fori_loop(first, last, body, 0)

    def mixing():
        def body(i, _):
            pair = i // 2
            top = pl.multiple_of((i % 2) * 512, 512)
            lanes = pl.ds(pl.multiple_of(pair * 128, 128), 128)
            m = mix_matrix[pl.ds(pair * 2, 2)].astype(BF).reshape(256, 128)
            v = jnp.concatenate(
                [vn[pl.ds(top + b * 128, 128), lanes] for b in range(4)], axis=1
            )
            both = jnp.dot(m, v, preferred_element_type=F32)
            low = lax.broadcasted_iota(jnp.int32, (128, 128), 1) < 64
            for b in range(4):
                rows = pl.ds(top + b * 128, 128)
                at = slice(b * 128, (b + 1) * 128)
                mixed = jnp.where(low, both[:128, at], both[128:, at]) + bias[:, lanes]
                gated[rows, lanes] = (acc[rows, lanes] * mixed).astype(BF)
            return 0
        lax.fori_loop(0, 8, body, 0)

    def out_part(first, last):
        for q in range(4):
            def body(i, _):
                rows = row_block(i)
                w = gathered_rows(buf, 2, q * 8, 8)
                part[rows, q * 512 : (q + 1) * 512] = dot_nt(gated[rows, :], w).astype(BF)
                return 0
            lax.fori_loop(first, last, body, 0)

    def spread_scales():
        low = lax.broadcasted_iota(jnp.int32, (1, 128), 1) < 64
        for s in range(0, SHARDS, 2):
            a, b = sbuf[place(SCALE_ORDER, s)], sbuf[place(SCALE_ORDER, s + 1)]
            at = slice(s * 64, s * 64 + 128)
            scales[0:1, at] = jnp.where(low, a, pltpu.roll(b, 64, 1))
            scales[1:2, at] = jnp.where(low, pltpu.roll(a, 64, 1), b)

    def middle(first, last):
        def body(i, _):
            rows = pl.ds(pl.multiple_of(i * EB, EB), EB)
            mix = (part[rows, :].astype(F32) + part_in[rows, :].astype(F32)) * scales[0:1, :]
            inv = lax.rsqrt(jnp.sum(mix * mix, axis=1, keepdims=True) / WIDTH + 1e-06)
            x_all = jnp.concatenate(
                [xfull[0, rows, :].astype(F32), xfull[1, rows, :].astype(F32)], axis=1
            )
            value = (x_all + mix * inv * gain_out[...]).astype(BF)
            xfull[0, rows, :] = value[:, :HALF]
            xfull[1, rows, :] = value[:, HALF:]
            wide = value.astype(F32)
            power = jnp.sum(wide * wide, axis=1, keepdims=True)
            nbuf[rows, :] = (wide * lax.rsqrt(power / WIDTH + 1e-06) * gain_up[...]).astype(BF)
            return 0
        lax.fori_loop(first, last, body, 0)

    def up_part(j, first, last):
        def body(i, _):
            rows = row_block(i)
            w = gathered_rows(buf, 3 + 2 * j)
            raised = jnp.dot(nbuf[rows, :], w, preferred_element_type=F32)
            raised = jnp.maximum(raised * up_scale[:, j * COLS : (j + 1) * COLS], 0.0)
            hid[rows, :] = (raised * raised).astype(BF)
            return 0
        lax.fori_loop(first, last, body, 0)

    def down_part(j, first, last):
        for q in range(4):
            def body(i, _):
                rows = row_block(i)
                w = gathered_rows(buf, 4 + 2 * j, q * 8, 8)
                at = slice(q * 512, (q + 1) * 512)
                term = dot_nt(hid[rows, :], w)
                acc[rows, at] = term if j == 0 else acc[rows, at] + term
                return 0
            lax.fori_loop(first, last, body, 0)

    own_cols = pl.ds(pl.multiple_of(lane * HALF, HALF), HALF)
    other_cols = pl.ds(pl.multiple_of((1 - lane) * HALF, HALF), HALF)

    def halves(i):
        def body(n, _):
            rows = pl.ds(pl.multiple_of(i * RB + n * EB, EB), EB)
            terms[rows, :] = acc[rows, other_cols].astype(BF)
            return 0
        lax.fori_loop(0, RB // EB, body, 0)

    def total_out(i):
        def body(n, _):
            rows = pl.ds(pl.multiple_of(i * RB + n * EB, EB), EB)
            own = acc[rows, own_cols].astype(BF).astype(F32)
            value = (own + terms_in[rows, :].astype(F32)) * scales[1:2, own_cols]
            acc[rows, own_cols] = value
            power = jnp.sum(value * value, axis=1, keepdims=True)
            stats[1, rows, :] = jnp.broadcast_to(power, (EB, 128))
            return 0
        lax.fori_loop(0, RB // EB, body, 0)

    def last_norm(i):
        def body(n, _):
            rows = pl.ds(pl.multiple_of(i * RB + n * EB, EB), EB)
            power = stats[1, rows, 0:1] + stats_in[1, rows, 0:1]
            inv = lax.rsqrt(power / WIDTH + 1e-06)
            value = acc[rows, own_cols] * inv * gain_last[:, own_cols]
            mid[rows, :] = (xfull[lane, rows, :].astype(F32) + value).astype(BF)
            return 0
        lax.fori_loop(0, RB // EB, body, 0)

    pending = []

    def exchange(src, dst, index):
        copy = to_partner(src, dst, index)
        copy.start()
        pending.append(copy)
        return copy

    waits = {}

    def stats_send():
        waits["stats"] = exchange(stats.at[0], stats_in.at[0], 0)

    def part_send(i):
        rows = pl.ds(i * RB, RB)
        waits["part", i] = exchange(part.at[rows], part_in.at[rows], 1 + i)

    def out_and_send(first, last):
        out_part(first, last)
        for i in range(first, last):
            part_send(i)

    def middle_of(first, last):
        for i in range(first, last):
            waits["part", i].wait_recv()
            middle(i * (RB // EB), (i + 1) * (RB // EB))

    def v_mixed():
        waits["stats"].wait_recv()
        v_normed(0, ROWS // EB)

    def compute(t):
        c = t - 6
        if c < 0:
            return {
                1: [(lambda: scales_step(t))],
                3: [x_normed] if t == 2 else [],
            }
        first, second = [], []
        if c == 0:
            first.append(lambda: arrived(0, 4))
            first.append(lambda: u_part(0, 2))
            second.append(lambda: u_part(2, 4))
        elif c == 1:
            first.append(lambda: arrived(1, 4))
            first.append(lambda: v_part(0, 2))
            second.append(lambda: v_part(2, 4))
            second.append(stats_send)
        elif c == 2:
            first.append(lambda: v_mixed())
            first.append(mixing)
            second.append(lambda: arrived(2, 4))
            second.append(lambda: out_and_send(0, 2))
            second.append(lambda: out_and_send(2, 4))
        elif c == 3:
            first.append(lambda: middle_of(0, 4))
            second.append(lambda: arrived(3, 4))
            second.append(lambda: up_part(0, 0, 4))
        elif c % 2 == 1:
            j = (c - 3) // 2
            first.append(lambda: arrived(c, 4))
            first.append(lambda: up_part(j, 0, 2))
            second.append(lambda: up_part(j, 2, 4))
        elif c < NCH - 1:
            j = (c - 4) // 2
            first.append(lambda: arrived(c, 4))
            first.append(lambda: down_part(j, 0, 2))
            second.append(lambda: down_part(j, 2, 4))
        return {1: first, 3: second}

    def scales_step(t):
        if t < STEPS:
            if t == 0:
                block = sbuf.at[0]
                pltpu.make_async_copy(block, block, load_sem.at[NCH]).wait()
            else:
                scales_arrived(t - 1)
            send_scales(t)
        else:
            scales_arrived(STEPS - 1)
            spread_scales()

    for t in range(NCH + 5):
        work = compute(t)
        for k in range(STEPS):
            substep(t, k)
            for job in work.get(k, []):
                job()

    arrived(NCH - 1, 4)
    for i in range(NRB):
        down_part(3, i, i + 1)
        halves(i)
        rows = pl.ds(i * RB, RB)
        waits["terms", i] = exchange(terms.at[rows], terms_in.at[rows], 5 + i)
    for i in range(NRB):
        waits["terms", i].wait_recv()
        total_out(i)
        rows = pl.ds(i * RB, RB)
        waits["power", i] = exchange(stats.at[1, rows], stats_in.at[1, rows], 9 + i)
    outs = []
    for i in range(NRB):
        waits["power", i].wait_recv()
        last_norm(i)
        rows = pl.ds(i * RB, RB)
        copy = pltpu.make_async_copy(mid.at[rows], result.at[rows], out_sem.at[i])
        copy.start()
        outs.append(copy)
    for copy in outs:
        copy.wait()
    for copy in pending:
        copy.wait_send()
    for c in range(NCH):
        block = buf.at[c, :, pl.ds(0, 31)]
        pltpu.make_async_copy(block, block, send_sem.at[c]).wait()
    for k in range(STEPS):
        block = sbuf.at[pl.ds(0, 1 << k)]
        pltpu.make_async_copy(block, block, s_send.at[k]).wait()


def set_of_orders():
    return sorted({*ORDERS[0], *ORDERS[1], SCALE_ORDER})


def local(
    resid,
    gain_mix_in,
    u_weight,
    v_weight,
    u_scale,
    v_scale,
    v_gain,
    mix_matrix,
    mix_bias,
    out_weight,
    out_scale,
    gain_mix_out,
    gain_ffn_in,
    up_weight,
    up_scale,
    down_weight,
    down_scale,
    gain_ffn_out,
):
    up = up_weight.reshape(64, 4, COLS).transpose(1, 0, 2)
    down = down_weight.T.reshape(64, 4, COLS).transpose(1, 0, 2)
    inner = jnp.stack([up, down], axis=1).reshape(8, 64, COLS)
    chunks = jnp.concatenate([jnp.stack([u_weight, v_weight, out_weight.T]), inner]).astype(BF)
    pieces = chunks.reshape(NCH, GROUPS_OF_ROWS, TILE, COLS)
    own_scales = jnp.concatenate([out_scale, down_scale]).reshape(1, 128)
    bias = jnp.repeat(mix_bias.T, 64, axis=1)
    row = lambda a: a.reshape(1, -1)
    vmem = pl.BlockSpec(memory_space=pltpu.VMEM)
    hbm = pl.BlockSpec(memory_space=pl.ANY)
    dma = pltpu.SemaphoreType.DMA
    return pl.pallas_call(
        kernel,
        out_shape=jax.ShapeDtypeStruct((ROWS, HALF), BF),
        in_specs=[hbm, hbm, hbm] + [vmem] * 10,
        out_specs=hbm,
        scratch_shapes=[
            pltpu.VMEM((NCH, GROUPS_OF_ROWS, SHARDS, TILE, COLS), BF),
            pltpu.VMEM((SHARDS, 1, 128), F32),
            pltpu.VMEM((2, WIDTH), F32),
            pltpu.VMEM((2, ROWS, HALF), BF),
            pltpu.VMEM((ROWS, WIDTH), BF),
            pltpu.VMEM((ROWS, WIDTH), F32),
            pltpu.VMEM((ROWS, COLS), BF),
            pltpu.VMEM((ROWS, COLS), BF),
            pltpu.VMEM((ROWS, WIDTH), BF),
            pltpu.VMEM((ROWS, WIDTH), BF),
            pltpu.VMEM((ROWS, HALF), BF),
            pltpu.VMEM((ROWS, COLS), BF),
            pltpu.VMEM((ROWS, HALF), BF),
            pltpu.VMEM((ROWS, HALF), BF),
            pltpu.VMEM((2, ROWS, 128), F32),
            pltpu.VMEM((2, ROWS, 128), F32),
            dma((NCH + 1,)),
            dma((NCH,)),
            dma((NCH, STEPS)),
            dma((STEPS,)),
            dma((STEPS,)),
            dma((3,)),
            dma((13,)),
            dma((13,)),
            dma((NRB,)),
        ],
        compiler_params=pltpu.CompilerParams(
            collective_id=0, has_side_effects=True, vmem_limit_bytes=67043328
        ),
    )(
        pieces,
        resid,
        own_scales,
        row(gain_mix_in),
        row(gain_mix_out),
        row(gain_ffn_in),
        row(gain_ffn_out),
        row(u_scale),
        row(v_scale),
        row(v_gain),
        mix_matrix,
        bias,
        row(up_scale),
    )


def solution(mesh):
    in_specs = (
        P(("rep", "fs"), "tp"),
        P(),
        P("fs", "tp"),
        P("fs", "tp"),
        P("tp"),
        P("tp"),
        P("tp"),
        P("tp", None, None),
        P("tp", None),
        P("tp", "fs"),
        P("fs"),
        P(),
        P(),
        P("fs", "tp"),
        P("tp"),
        P("tp", "fs"),
        P("fs"),
        P(),
    )
    out_specs = P(("rep", "fs"), "tp")
    return jax.shard_map(local, mesh=mesh, in_specs=in_specs, out_specs=out_specs, check_vma=False)
```

```python
import itertools

import jax
import jax.numpy as jnp
from jax import lax
from jax.experimental import pallas as pl
from jax.experimental.pallas import tpu as pltpu
from jax.sharding import PartitionSpec as P

MESH = pl.DeviceIdType.MESH
BF = jnp.bfloat16
F32 = jnp.float32

ROWS = 1024
WIDTH = 2048
HALF = 1024
COLS = 512
NCH = 11
STEPS = 5
SHARDS = 32
TILE = 16
PARTS = 4
RB = 256
NRB = ROWS // RB
MB = 512
EB = 32

CROSSINGS = [
    order
    for z in ("S", "O")
    for order in itertools.permutations(("PX", "QX", "PY", "QY", z))
]
ORDERS = (
    (24, 123, 198, 39),
    (88, 195, 178, 80),
    (49, 95, 150, 78),
    (197, 183, 132, 126),
    (78, 36, 111, 7),
    (182, 153, 108, 63),
    (12, 129, 27, 66),
    (5, 173, 194, 192),
    (12, 142, 48, 111),
    (42, 75, 156, 158),
    (76, 12, 35, 169),
)
SCALE_ORDER = ("PX", "QY", "QX", "PY", "S")
PROGRAM = (
    0, 1, 2, 3, 20, 21, 22, 23, 40, 41, 42, 43, 61, 62, 63, 81, 82, 83, 100, 101,
    102, 103, 120, 60, 121, 122, 123, 140, 141, 163, 180, 182, 160, 80, 162, 183, 161, 142, 203, 202,
    201, 143, 181, 200, 4, 5, 6, 26, 7, 66, 24, 86, 44, 46, 25, 65, 67, 27, 45, 85,
    87, 126, 47, 127, 184, 64, 144, 104, 145, 105, 165, 84, 146, 107, 106, 147, 124, 125, 28, 166,
    9, 8, 48, 220, 10, 30, 70, 164, 221, 11, 50, 68, 69, 130, 222, 29, 51, 71, 109, 148,
    149, 223, 31, 32, 90, 52, 129, 49, 13, 91, 12, 14, 15, 108, 34, 73, 111, 54, 134, 33,
    55, 128, 35, 53, 75, 95, 113, 167, 88, 17, 36, 89, 186, 16, 187, 18, 110, 38, 19, 72,
    37, 39, 58, 94, 74, 131, 185, 205, 92, 204, 56, 151, 207, 59, 57, 79, 114, 93, 224, 225,
    150, 168, 226, 206, 112, 115, 169, 170, 78, 132, 99, 227, 171, 76, 96, 77, 189, 191, 228, 133,
    152, 155, 229, 135, 188, 97, 230, 190, 153, 116, 172, 231, 98, 154, 118, 138, 232, 233, 208, 209,
    211, 159, 210, 173, 136, 117, 192, 174, 234, 137, 235, 175, 194, 158, 236, 119, 193, 237, 139, 156,
    238, 157, 176, 239, 215, 240, 195, 213, 214, 198, 241, 212, 178, 179, 177, 196, 242, 197, 243, 199,
    244, 217, 218, 219, 245, 216, 246, 247, 248, 249, 250, 251, 252, 253,
)
JOB_NAMES = (
    ["xn0", "xn1", "xn2", "xn3", "u0", "u1", "v0", "v1", "mix0", "mix1", "mix2", "mix3"]
    + ["out0", "out1", "mid0", "mid1", "mid2", "mid3"]
    + [f"{kind}{j}{i}" for j in range(4) for kind in ("up", "dn") for i in range(2)]
)


def link_bits(fs):
    x, y, z = fs % 4, (fs // 4) % 4, fs // 16
    return {
        "PX": (x + x // 2) % 2,
        "QX": x // 2,
        "PY": (y + y // 2) % 2,
        "QY": y // 2,
        "S": z,
        "O": z,
    }


def place(order, fs):
    bits = link_bits(fs)
    return sum(bits[name] * (1 << k) for k, name in enumerate(order))


def order_of(c, r):
    return CROSSINGS[ORDERS[c][r]]


def gathered_rows(buf, c, first=0, count=SHARDS):
    return jnp.concatenate(
        [
            buf[c, r, place(order_of(c, r), s)]
            for s in range(first, first + count)
            for r in range(PARTS)
        ],
        axis=0,
    )


def rows_of_half(buf, c, half, first, count):
    blocks = []
    for s in range(first, first + count):
        for r in range(PARTS):
            order = order_of(c, r)
            step = max(order.index(z) for z in ("S", "O") if z in order)
            blocks.append(buf[c, r, place(order, s) + half * (1 << step)])
    return jnp.concatenate(blocks, axis=0)


def dot_nt(a, b):
    return lax.dot_general(a, b, (((1,), (1,)), ((), ())), preferred_element_type=F32)


def kernel(
    u_weight,
    v_weight,
    out_weight,
    up_weight,
    down_weight,
    resid,
    mix_matrix,
    out_scale,
    down_scale,
    gain_in,
    gain_out,
    gain_up,
    gain_last,
    u_scale,
    v_scale,
    v_gain,
    mix_bias,
    up_scale,
    result,
    wide,
    buf,
    sbuf,
    scales,
    mix,
    bias,
    xfull,
    nbuf,
    acc,
    vn,
    gated,
    part,
    part_in,
    mid,
    hid,
    terms,
    terms_in,
    stats,
    stats_in,
    load_sem,
    send_sem,
    recv_sem,
    s_send,
    s_recv,
    x_sem,
    pair_send,
    pair_recv,
    out_sem,
):
    rep, fs, lane = lax.axis_index("rep"), lax.axis_index("fs"), lax.axis_index("tp")
    x, y, z = fs % 4, (fs // 4) % 4, fs // 16
    here = z * 16 + y * 4
    far = (1 - z) * 16 + y * 4 + x
    peer = {
        "PX": (rep, here + x + 1 - 2 * (x % 2), lane),
        "QX": (rep, here + 3 - x, lane),
        "PY": (rep, z * 16 + (y + 1 - 2 * (y % 2)) * 4 + x, lane),
        "QY": (rep, z * 16 + (3 - y) * 4 + x, lane),
        "S": (rep, far, lane),
        "O": (1 - rep, far, lane),
    }
    partner = (rep, fs, 1 - lane)
    used = sorted({order_of(c, r) for c in range(NCH) for r in range(PARTS)} | {SCALE_ORDER})
    places = {order: place(order, fs) for order in used}

    barrier = pltpu.get_barrier_semaphore()
    for device in (*peer.values(), partner):
        pl.semaphore_signal(barrier, inc=1, device_id=device, device_id_type=MESH)

    loads = []
    at = 0
    for n, source in enumerate((u_weight, v_weight, out_weight, up_weight, down_weight)):
        span = source.shape[1]
        copy = pltpu.make_async_copy(source, wide.at[:, at : at + span], load_sem.at[n])
        copy.start()
        loads.append(copy)
        at += span
    own_x = pltpu.make_async_copy(resid, xfull.at[lane], x_sem.at[0])
    own_x.start()
    own_mix = pltpu.make_async_copy(mix_matrix, mix, load_sem.at[5])
    own_mix.start()

    def narrow(c, first):
        for r in range(PARTS):
            value = wide[r * TILE : (r + 1) * TILE, first : first + COLS]
            buf[c, r, places[order_of(c, r)]] = value.astype(BF)

    for n in range(3):
        loads[n].wait()
        narrow(n, n * COLS)
    for n in range(2):
        loads[3 + n].wait()
        for j in range(4):
            narrow(3 + 2 * j + n, 3 * COLS + n * WIDTH + j * COLS)
    sbuf[places[SCALE_ORDER], 0:1, 0:64] = out_scale[...]
    sbuf[places[SCALE_ORDER], 1:2, 0:64] = down_scale[...]

    pl.semaphore_wait(barrier, 7)

    other_x = pltpu.make_async_remote_copy(
        src_ref=resid,
        dst_ref=xfull.at[lane],
        send_sem=x_sem.at[1],
        recv_sem=x_sem.at[2],
        device_id=partner,
        device_id_type=MESH,
    )
    other_x.start()

    def send(c, k, r):
        size = 1 << k
        order = order_of(c, r)
        block = buf.at[c, r, pl.ds((places[order] // size) * size, size)]
        pltpu.make_async_remote_copy(
            src_ref=block,
            dst_ref=block,
            send_sem=send_sem.at[c],
            recv_sem=recv_sem.at[c, k, r],
            device_id=peer[order[k]],
            device_id_type=MESH,
        ).start()

    def arrived(c, k, r):
        block = buf.at[c, r, pl.ds(0, 1 << k)]
        pltpu.make_async_copy(block, block, recv_sem.at[c, k, r]).wait()

    complete = set()

    def chunk(c):
        if c not in complete:
            complete.add(c)
            for r in range(PARTS):
                arrived(c, STEPS - 1, r)

    def send_scales(k):
        size = 1 << k
        block = sbuf.at[pl.ds((places[SCALE_ORDER] // size) * size, size)]
        pltpu.make_async_remote_copy(
            src_ref=block,
            dst_ref=block,
            send_sem=s_send.at[k],
            recv_sem=s_recv.at[k],
            device_id=peer[SCALE_ORDER[k]],
            device_id_type=MESH,
        ).start()

    def scales_arrived(k):
        block = sbuf.at[pl.ds(0, 1 << k)]
        pltpu.make_async_copy(block, block, s_recv.at[k]).wait()

    def spread_scales():
        low = lax.broadcasted_iota(jnp.int32, (1, 128), 1) < 64
        for n in range(2):
            for s in range(0, SHARDS, 2):
                a = sbuf[place(SCALE_ORDER, s), n : n + 1, :]
                b = sbuf[place(SCALE_ORDER, s + 1), n : n + 1, :]
                scales[n : n + 1, s * 64 : s * 64 + 128] = jnp.where(low, a, pltpu.roll(b, 64, 1))

    pending, waits, waited = [], {}, set()

    def exchange(src, dst, index, name):
        copy = pltpu.make_async_remote_copy(
            src_ref=src,
            dst_ref=dst,
            send_sem=pair_send.at[index],
            recv_sem=pair_recv.at[index],
            device_id=partner,
            device_id_type=MESH,
        )
        copy.start()
        pending.append(copy)
        waits[name] = copy

    def received(name):
        if name not in waited:
            waited.add(name)
            waits[name].wait_recv()

    def in_rows(first, count, size, body):
        def step(i, carry):
            body(pl.ds(pl.multiple_of(first + i * size, size), size))
            return carry

        lax.fori_loop(0, count // size, step, 0)

    def spread_bias():
        turned = jnp.concatenate([mix_bias[...]] * 16, axis=0).T
        low = lax.broadcasted_iota(jnp.int32, (128, 128), 1) < 64
        for pair in range(4):
            bias[:, pair * 128 : (pair + 1) * 128] = jnp.where(
                low, turned[:, 2 * pair : 2 * pair + 1], turned[:, 2 * pair + 1 : 2 * pair + 2]
            )

    def job_xn(i):
        if i == 0:
            spread_bias()
            own_x.wait()
            other_x.wait()

        def body(rows):
            a = xfull[0, rows, :].astype(F32)
            b = xfull[1, rows, :].astype(F32)
            power = jnp.sum(a * a, axis=1, keepdims=True) + jnp.sum(b * b, axis=1, keepdims=True)
            inv = lax.rsqrt(power / WIDTH + 1e-06)
            nbuf[rows, :HALF] = (a * inv * gain_in[:, :HALF]).astype(BF)
            nbuf[rows, HALF:] = (b * inv * gain_in[:, HALF:]).astype(BF)

        in_rows(i * RB, RB, EB, body)

    def job_u(i):
        chunk(0)
        rows = slice(i * MB, (i + 1) * MB)
        pre = jnp.dot(nbuf[rows, :], gathered_rows(buf, 0), preferred_element_type=F32)
        acc[0, rows, :COLS] = jax.nn.gelu(pre * u_scale[...])

    def job_v(i):
        chunk(1)
        rows = slice(i * MB, (i + 1) * MB)
        pre = jnp.dot(nbuf[rows, :], gathered_rows(buf, 1), preferred_element_type=F32)
        act = jax.nn.gelu(pre * v_scale[...])
        acc[0, rows, COLS:] = act
        total = jnp.sum(act, axis=1, keepdims=True)
        off = act - total / COLS
        spread = jnp.sum(off * off, axis=1, keepdims=True)
        lanes = lax.broadcasted_iota(jnp.int32, (MB, 128), 1)
        stats[0, rows, :] = jnp.where(lanes == 0, total, spread)
        exchange(stats.at[0, pl.ds(i * MB, MB)], stats_in.at[0, pl.ds(i * MB, MB)], i, f"v{i}")

    def job_mix(i):
        received(f"v{i // 2}")
        if i == 0:
            own_mix.wait()

        def body(rows):
            act = acc[0, rows, COLS:]
            own, other = stats[0, rows, :], stats_in[0, rows, :]
            total = own[:, 0:1] + other[:, 0:1]
            apart = (own[:, 0:1] - other[:, 0:1]) / COLS
            spread = own[:, 1:2] + other[:, 1:2] + apart * apart * (COLS / 2)
            centre = total / (2 * COLS)
            inv = lax.rsqrt(spread / (2 * COLS) + 1e-06)
            vn[rows, :] = ((act - centre) * inv * v_gain[...]).astype(BF)

        in_rows(i * RB, RB, 64, body)
        low = lax.broadcasted_iota(jnp.int32, (128, 128), 1) < 64
        for pair in range(4):
            lanes = slice(pair * 128, (pair + 1) * 128)
            m = mix[2 * pair : 2 * pair + 2].astype(BF).reshape(256, 128)
            v = jnp.concatenate(
                [vn[i * RB + b * 128 : i * RB + (b + 1) * 128, lanes] for b in range(2)], axis=1
            )
            both = jnp.dot(m, v, preferred_element_type=F32)
            for b in range(2):
                rows = slice(i * RB + b * 128, i * RB + (b + 1) * 128)
                span = slice(b * 128, (b + 1) * 128)
                mixed = jnp.where(low, both[:128, span], both[128:, span]) + bias[:, lanes]
                gated[rows, lanes] = (acc[0, rows, lanes] * mixed).astype(BF)

    def job_out(i):
        chunk(2)
        rows = slice(i * MB, (i + 1) * MB)
        for q in range(4):
            w = gathered_rows(buf, 2, q * 8, 8)
            part[rows, q * COLS : (q + 1) * COLS] = dot_nt(gated[rows, :], w).astype(BF)
        for n in (2 * i, 2 * i + 1):
            block = pl.ds(n * RB, RB)
            exchange(part.at[block], part_in.at[block], 2 + n, f"out{n}")

    def job_mid(i):
        received(f"out{i}")

        def body(rows):
            total = (part[rows, :].astype(F32) + part_in[rows, :].astype(F32)) * scales[0:1, :]
            inv = lax.rsqrt(jnp.sum(total * total, axis=1, keepdims=True) / WIDTH + 1e-06)
            stream = jnp.concatenate(
                [xfull[0, rows, :].astype(F32), xfull[1, rows, :].astype(F32)], axis=1
            )
            value = (stream + total * inv * gain_out[...]).astype(BF)
            xfull[0, rows, :] = value[:, :HALF]
            xfull[1, rows, :] = value[:, HALF:]
            again = value.astype(F32)
            power = jnp.sum(again * again, axis=1, keepdims=True)
            nbuf[rows, :] = (again * lax.rsqrt(power / WIDTH + 1e-06) * gain_up[...]).astype(BF)

        in_rows(i * RB, RB, EB, body)

    def job_up(j, i):
        c = 3 + 2 * j
        chunk(c)
        rows = slice(i * MB, (i + 1) * MB)
        raised = jnp.dot(nbuf[rows, :], gathered_rows(buf, c), preferred_element_type=F32)
        raised = jnp.maximum(raised * up_scale[:, j * COLS : (j + 1) * COLS], 0.0)
        hid[rows, :] = (raised * raised).astype(BF)

    def job_dn(j, i):
        c = 4 + 2 * j
        chunk(c)
        rows = slice(i * MB, (i + 1) * MB)
        for q in range(4):
            span = slice((q % 2) * COLS, (q % 2 + 1) * COLS)
            term = dot_nt(hid[rows, :], gathered_rows(buf, c, q * 8, 8))
            acc[q // 2, rows, span] = term if j == 0 else acc[q // 2, rows, span] + term

    def last_down(half, i):
        rows = slice(i * MB, (i + 1) * MB)
        for q in range(2):
            span = slice(q * COLS, (q + 1) * COLS)
            term = dot_nt(hid[rows, :], rows_of_half(buf, NCH - 1, half, q * 8, 8))
            yield rows, span, (acc[half, rows, span] + term).astype(BF)

    def job(name):
        kind, index = name.rstrip("0123456789"), [int(n) for n in name[len(name.rstrip("0123456789")) :]]
        {"xn": job_xn, "u": job_u, "v": job_v, "mix": job_mix, "out": job_out, "mid": job_mid, "up": job_up, "dn": job_dn}[kind](*index)

    send_scales(0)
    turns = {50: 1, 90: 2, 120: 3, 150: 4, 165: 5}
    for n, code in enumerate(PROGRAM):
        if n in turns:
            scales_arrived(turns[n] - 1)
            if turns[n] < STEPS:
                send_scales(turns[n])
            else:
                spread_scales()
        if code >= 220:
            name = JOB_NAMES[code - 220]
            if not name.startswith("dn3"):
                job(name)
        else:
            c, k, r = code // 20, (code // 4) % 5, code % 4
            if k:
                arrived(c, k - 1, r)
            send(c, k, r)

    chunk(NCH - 1)
    own, other = lane, 1 - lane
    for i in range(2):
        for rows, span, value in last_down(other, i):
            terms[rows, span] = value
        for n in (2 * i, 2 * i + 1):
            block = pl.ds(n * RB, RB)
            exchange(terms.at[block], terms_in.at[block], 6 + n, f"terms{n}")
    for i in range(2):
        for rows, span, value in last_down(own, i):
            acc[own, rows, span] = value.astype(F32)
    own_cols = pl.ds(pl.multiple_of(lane * HALF, HALF), HALF)

    def add_up(rows):
        value = (acc[own, rows, :] + terms_in[rows, :].astype(F32)) * scales[1:2, own_cols]
        acc[own, rows, :] = value
        power = jnp.sum(value * value, axis=1, keepdims=True)
        stats[1, rows, :] = jnp.broadcast_to(power, (EB, 128))

    def finish(rows):
        power = stats[1, rows, 0:1] + stats_in[1, rows, 0:1]
        inv = lax.rsqrt(power / WIDTH + 1e-06)
        value = acc[own, rows, :] * inv * gain_last[:, own_cols]
        mid[rows, :] = (xfull[lane, rows, :].astype(F32) + value).astype(BF)

    for i in range(NRB):
        received(f"terms{i}")
        in_rows(i * RB, RB, EB, add_up)
        block = pl.ds(i * RB, RB)
        exchange(stats.at[1, block], stats_in.at[1, block], 10 + i, f"power{i}")
    outs = []
    for i in range(NRB):
        received(f"power{i}")
        in_rows(i * RB, RB, EB, finish)
        block = pl.ds(i * RB, RB)
        copy = pltpu.make_async_copy(mid.at[block], result.at[block], out_sem.at[i])
        copy.start()
        outs.append(copy)
    for copy in outs:
        copy.wait()
    for copy in pending:
        copy.wait_send()
    for c in range(NCH):
        block = buf.at[c, :, pl.ds(0, 31)]
        pltpu.make_async_copy(block, block, send_sem.at[c]).wait()
    for k in range(STEPS):
        block = sbuf.at[pl.ds(0, 1 << k)]
        pltpu.make_async_copy(block, block, s_send.at[k]).wait()


def local(
    resid,
    gain_mix_in,
    u_weight,
    v_weight,
    u_scale,
    v_scale,
    v_gain,
    mix_matrix,
    mix_bias,
    out_weight,
    out_scale,
    gain_mix_out,
    gain_ffn_in,
    up_weight,
    up_scale,
    down_weight,
    down_scale,
    gain_ffn_out,
):
    row = lambda a: a.reshape(1, -1)
    vmem = pl.BlockSpec(memory_space=pltpu.VMEM)
    hbm = pl.BlockSpec(memory_space=pl.ANY)
    dma = pltpu.SemaphoreType.DMA
    return pl.pallas_call(
        kernel,
        out_shape=jax.ShapeDtypeStruct((ROWS, HALF), BF),
        in_specs=[hbm] * 7 + [vmem] * 11,
        out_specs=hbm,
        scratch_shapes=[
            pltpu.VMEM((64, 3 * COLS + 2 * WIDTH), F32),
            pltpu.VMEM((NCH, PARTS, SHARDS, TILE, COLS), BF),
            pltpu.VMEM((SHARDS, 2, 128), F32),
            pltpu.VMEM((2, WIDTH), F32),
            pltpu.VMEM((8, 128, 128), F32),
            pltpu.VMEM((128, COLS), F32),
            pltpu.VMEM((2, ROWS, HALF), BF),
            pltpu.VMEM((ROWS, WIDTH), BF),
            pltpu.VMEM((2, ROWS, HALF), F32),
            pltpu.VMEM((ROWS, COLS), BF),
            pltpu.VMEM((ROWS, COLS), BF),
            pltpu.VMEM((ROWS, WIDTH), BF),
            pltpu.VMEM((ROWS, WIDTH), BF),
            pltpu.VMEM((ROWS, HALF), BF),
            pltpu.VMEM((ROWS, COLS), BF),
            pltpu.VMEM((ROWS, HALF), BF),
            pltpu.VMEM((ROWS, HALF), BF),
            pltpu.VMEM((2, ROWS, 128), F32),
            pltpu.VMEM((2, ROWS, 128), F32),
            dma((6,)),
            dma((NCH,)),
            dma((NCH, STEPS, PARTS)),
            dma((STEPS,)),
            dma((STEPS,)),
            dma((3,)),
            dma((14,)),
            dma((14,)),
            dma((NRB,)),
        ],
        compiler_params=pltpu.CompilerParams(
            collective_id=0, has_side_effects=True, vmem_limit_bytes=67043328
        ),
    )(
        u_weight,
        v_weight,
        out_weight.T,
        up_weight,
        down_weight.T,
        resid,
        mix_matrix,
        row(out_scale),
        row(down_scale),
        row(gain_mix_in),
        row(gain_mix_out),
        row(gain_ffn_in),
        row(gain_ffn_out),
        row(u_scale),
        row(v_scale),
        row(v_gain),
        mix_bias,
        row(up_scale),
    )


def solution(mesh):
    in_specs = (
        P(("rep", "fs"), "tp"),
        P(),
        P("fs", "tp"),
        P("fs", "tp"),
        P("tp"),
        P("tp"),
        P("tp"),
        P("tp", None, None),
        P("tp", None),
        P("tp", "fs"),
        P("fs"),
        P(),
        P(),
        P("fs", "tp"),
        P("tp"),
        P("tp", "fs"),
        P("fs"),
        P(),
    )
    out_specs = P(("rep", "fs"), "tp")
    return jax.shard_map(local, mesh=mesh, in_specs=in_specs, out_specs=out_specs, check_vma=False)
```

```python
import itertools

import jax
import jax.numpy as jnp
from jax import lax
from jax.experimental import pallas as pl
from jax.experimental.pallas import tpu as pltpu
from jax.sharding import PartitionSpec as P

MESH = pl.DeviceIdType.MESH
BF = jnp.bfloat16
F32 = jnp.float32

ROWS = 1024
WIDTH = 2048
HALF = 1024
COLS = 512
NCH = 11
STEPS = 5
SHARDS = 32
TILE = 16
PARTS = 4
RB = 256
NRB = ROWS // RB
MB = 512
EB = 32
AT_ONCE = 2
VMEM_LIMIT = 56 * 1024 * 1024

CROSSINGS = [
    order
    for z in ("S", "O")
    for order in itertools.permutations(("PX", "QX", "PY", "QY", z))
]
ORDERS = (
    (58, 77, 30, 176),
    (126, 202, 51, 8),
    (63, 127, 5, 84),
    (146, 81, 206, 24),
    (80, 177, 161, 137),
    (194, 170, 6, 210),
    (172, 26, 194, 177),
    (72, 139, 62, 143),
    (5, 120, 41, 44),
    (185, 24, 126, 195),
    (47, 98, 5, 129),
)
SCALE_ORDER = ("PX", "QY", "QX", "PY", "S")
PROGRAM = (
    0, 1, 2, 3, 20, 21, 22, 23, 40, 41, 42, 43, 60, 61, 62, 63, 80, 81, 82, 83,
    100, 101, 102, 103, 120, 121, 123, 141, 142, 122, 143, 162, 160, 163, 181, 200, 180, 140, 201, 161,
    183, 182, 202, 203, 4, 6, 5, 24, 7, 25, 27, 26, 45, 44, 65, 86, 46, 64, 87, 47,
    166, 84, 67, 145, 167, 66, 107, 147, 146, 85, 104, 204, 106, 184, 220, 8, 10, 11, 48, 186,
    221, 9, 28, 29, 31, 105, 69, 124, 90, 222, 30, 49, 50, 51, 71, 91, 170, 223, 12, 68,
    70, 88, 188, 108, 89, 127, 52, 110, 13, 14, 15, 128, 73, 35, 53, 94, 32, 33, 34, 55,
    93, 72, 16, 125, 164, 126, 18, 17, 144, 19, 111, 95, 74, 37, 54, 36, 39, 92, 165, 38,
    109, 185, 75, 187, 56, 130, 224, 129, 58, 59, 76, 225, 131, 148, 149, 57, 150, 205, 77, 78,
    79, 112, 226, 207, 169, 227, 151, 113, 171, 133, 228, 114, 115, 168, 135, 97, 229, 96, 189, 153,
    230, 206, 132, 191, 152, 116, 231, 98, 208, 232, 134, 155, 118, 211, 233, 117, 172, 99, 119, 173,
    154, 234, 210, 136, 235, 175, 190, 137, 138, 236, 209, 139, 192, 174, 237, 238, 193, 159, 157, 239,
    195, 156, 240, 194, 241, 215, 178, 242, 212, 213, 214, 158, 177, 243, 244, 176, 179, 196, 199, 245,
    198, 197, 217, 219, 216, 218, 246, 247, 248, 249, 250, 251, 252, 253,
)
JOB_NAMES = (
    ["xn0", "xn1", "xn2", "xn3", "u0", "u1", "v0", "v1", "mix0", "mix1", "mix2", "mix3"]
    + ["out0", "out1", "mid0", "mid1", "mid2", "mid3"]
    + [f"{kind}{j}{i}" for j in range(4) for kind in ("up", "dn") for i in range(2)]
)


def link_bits(fs):
    x, y, z = fs % 4, (fs // 4) % 4, fs // 16
    return {
        "PX": (x + x // 2) % 2,
        "QX": x // 2,
        "PY": (y + y // 2) % 2,
        "QY": y // 2,
        "S": z,
        "O": z,
    }


def place(order, fs):
    bits = link_bits(fs)
    return sum(bits[name] * (1 << k) for k, name in enumerate(order))


def order_of(c, r):
    return CROSSINGS[ORDERS[c][r]]


def gathered_rows(buf, c, first=0, count=SHARDS):
    return jnp.concatenate(
        [
            buf[c, r, place(order_of(c, r), s)]
            for s in range(first, first + count)
            for r in range(PARTS)
        ],
        axis=0,
    )


def rows_of_half(buf, c, half, first, count):
    blocks = []
    for s in range(first, first + count):
        for r in range(PARTS):
            order = order_of(c, r)
            step = max(order.index(z) for z in ("S", "O") if z in order)
            blocks.append(buf[c, r, place(order, s) + half * (1 << step)])
    return jnp.concatenate(blocks, axis=0)


def dot_nt(a, b):
    return lax.dot_general(a, b, (((1,), (1,)), ((), ())), preferred_element_type=F32)


def kernel(
    u_weight,
    v_weight,
    out_weight,
    up_weight,
    down_weight,
    resid,
    mix_matrix,
    out_scale,
    down_scale,
    gain_in,
    gain_out,
    gain_up,
    gain_last,
    u_scale,
    v_scale,
    v_gain,
    mix_bias,
    up_scale,
    result,
    buf,
    sbuf,
    scales,
    mix,
    bias,
    xfull,
    nbuf,
    acc,
    vn,
    gated,
    part,
    part_in,
    terms_in,
    stats,
    stats_in,
    load_sem,
    send_sem,
    recv_sem,
    s_send,
    s_recv,
    x_sem,
    pair_send,
    pair_recv,
):
    rep, fs, lane = lax.axis_index("rep"), lax.axis_index("fs"), lax.axis_index("tp")
    x, y, z = fs % 4, (fs // 4) % 4, fs // 16
    here = z * 16 + y * 4
    far = (1 - z) * 16 + y * 4 + x
    peer = {
        "PX": (rep, here + x + 1 - 2 * (x % 2), lane),
        "QX": (rep, here + 3 - x, lane),
        "PY": (rep, z * 16 + (y + 1 - 2 * (y % 2)) * 4 + x, lane),
        "QY": (rep, z * 16 + (3 - y) * 4 + x, lane),
        "S": (rep, far, lane),
        "O": (1 - rep, far, lane),
    }
    partner = (rep, fs, 1 - lane)
    used = sorted({order_of(c, r) for c in range(NCH) for r in range(PARTS)} | {SCALE_ORDER})
    places = {order: place(order, fs) for order in used}

    barrier = pltpu.get_barrier_semaphore()
    for device in (*peer.values(), partner):
        pl.semaphore_signal(barrier, inc=1, device_id=device, device_id_type=MESH)

    loads = []

    def load(source, first, c, sem):
        slot = acc.at[0, pl.ds(c * 64, 64), pl.ds(0, COLS)]
        copy = pltpu.make_async_copy(source.at[:, pl.ds(first, COLS)], slot, load_sem.at[sem])
        copy.start()
        loads.append(copy)

    for n, source in enumerate((u_weight, v_weight, out_weight)):
        load(source, 0, n, n)
    for j in range(4):
        load(up_weight, j * COLS, 3 + 2 * j, 3 + 2 * j)
        load(down_weight, j * COLS, 4 + 2 * j, 4 + 2 * j)
    own_x = pltpu.make_async_copy(resid, xfull.at[lane], x_sem.at[0])
    own_x.start()
    own_mix = pltpu.make_async_copy(mix_matrix, mix, load_sem.at[NCH])
    own_mix.start()

    for c in range(NCH):
        loads[c].wait()
        for r in range(PARTS):
            value = acc[0, c * 64 + r * TILE : c * 64 + (r + 1) * TILE, :COLS]
            buf[c, r, places[order_of(c, r)]] = value.astype(BF)
    sbuf[places[SCALE_ORDER], 0:1, 0:64] = out_scale[...]
    sbuf[places[SCALE_ORDER], 1:2, 0:64] = down_scale[...]

    pl.semaphore_wait(barrier, 7)

    other_x = pltpu.make_async_remote_copy(
        src_ref=resid,
        dst_ref=xfull.at[lane],
        send_sem=x_sem.at[1],
        recv_sem=x_sem.at[2],
        device_id=partner,
        device_id_type=MESH,
    )
    other_x.start()

    def send(c, k, r):
        size = 1 << k
        order = order_of(c, r)
        block = buf.at[c, r, pl.ds((places[order] // size) * size, size)]
        pltpu.make_async_remote_copy(
            src_ref=block,
            dst_ref=block,
            send_sem=send_sem.at[c],
            recv_sem=recv_sem.at[c, k, r],
            device_id=peer[order[k]],
            device_id_type=MESH,
        ).start()

    def arrived(c, k, r):
        block = buf.at[c, r, pl.ds(0, 1 << k)]
        pltpu.make_async_copy(block, block, recv_sem.at[c, k, r]).wait()

    complete = set()

    def chunk(c):
        if c not in complete:
            complete.add(c)
            for r in range(PARTS):
                arrived(c, STEPS - 1, r)

    def send_scales(k):
        size = 1 << k
        block = sbuf.at[pl.ds((places[SCALE_ORDER] // size) * size, size)]
        pltpu.make_async_remote_copy(
            src_ref=block,
            dst_ref=block,
            send_sem=s_send.at[k],
            recv_sem=s_recv.at[k],
            device_id=peer[SCALE_ORDER[k]],
            device_id_type=MESH,
        ).start()

    def scales_arrived(k):
        block = sbuf.at[pl.ds(0, 1 << k)]
        pltpu.make_async_copy(block, block, s_recv.at[k]).wait()

    def spread_scales():
        low = lax.broadcasted_iota(jnp.int32, (1, 128), 1) < 64
        for n in range(2):
            for s in range(0, SHARDS, 2):
                a = sbuf[place(SCALE_ORDER, s), n : n + 1, :]
                b = sbuf[place(SCALE_ORDER, s + 1), n : n + 1, :]
                scales[n : n + 1, s * 64 : s * 64 + 128] = jnp.where(low, a, pltpu.roll(b, 64, 1))

    pending, waits, waited = {}, {}, set()

    def exchange(src, dst, index, name):
        copy = pltpu.make_async_remote_copy(
            src_ref=src,
            dst_ref=dst,
            send_sem=pair_send.at[index],
            recv_sem=pair_recv.at[index],
            device_id=partner,
            device_id_type=MESH,
        )
        copy.start()
        pending[name] = copy
        waits[name] = copy

    def received(name):
        if name not in waited:
            waited.add(name)
            waits[name].wait_recv()

    def sent(name):
        pending.pop(name).wait_send()

    def in_rows(first, count, size, body, at_once=1):
        def step(i, carry):
            for n in range(at_once):
                body(pl.ds(pl.multiple_of(first + (i * at_once + n) * size, size), size))
            return carry

        lax.fori_loop(0, count // (size * at_once), step, 0)

    def spread_bias():
        turned = jnp.concatenate([mix_bias[...]] * 16, axis=0).T
        low = lax.broadcasted_iota(jnp.int32, (128, 128), 1) < 64
        for pair in range(4):
            bias[:, pair * 128 : (pair + 1) * 128] = jnp.where(
                low, turned[:, 2 * pair : 2 * pair + 1], turned[:, 2 * pair + 1 : 2 * pair + 2]
            )

    def job_xn(i):
        if i == 0:
            spread_bias()
            own_x.wait()
            other_x.wait()

        def body(rows):
            a = xfull[0, rows, :].astype(F32)
            b = xfull[1, rows, :].astype(F32)
            power = jnp.sum(a * a, axis=1, keepdims=True) + jnp.sum(b * b, axis=1, keepdims=True)
            inv = lax.rsqrt(power / WIDTH + 1e-06)
            nbuf[rows, :HALF] = (a * inv * gain_in[:, :HALF]).astype(BF)
            nbuf[rows, HALF:] = (b * inv * gain_in[:, HALF:]).astype(BF)

        in_rows(i * RB, RB, EB, body, AT_ONCE)

    def job_u(i):
        chunk(0)
        rows = slice(i * MB, (i + 1) * MB)
        pre = jnp.dot(nbuf[rows, :], gathered_rows(buf, 0), preferred_element_type=F32)
        acc[0, rows, :COLS] = jax.nn.gelu(pre * u_scale[...])

    def job_v(i):
        chunk(1)
        rows = slice(i * MB, (i + 1) * MB)
        pre = jnp.dot(nbuf[rows, :], gathered_rows(buf, 1), preferred_element_type=F32)
        act = jax.nn.gelu(pre * v_scale[...])
        acc[0, rows, COLS:] = act
        total = jnp.sum(act, axis=1, keepdims=True)
        off = act - total / COLS
        spread = jnp.sum(off * off, axis=1, keepdims=True)
        lanes = lax.broadcasted_iota(jnp.int32, (MB, 128), 1)
        stats[0, rows, :] = jnp.where(lanes == 0, total, spread)
        exchange(stats.at[0, pl.ds(i * MB, MB)], stats_in.at[0, pl.ds(i * MB, MB)], i, f"v{i}")

    def job_mix(i):
        received(f"v{i // 2}")
        if i == 0:
            own_mix.wait()

        def body(rows):
            act = acc[0, rows, COLS:]
            own, other = stats[0, rows, :], stats_in[0, rows, :]
            total = own[:, 0:1] + other[:, 0:1]
            apart = (own[:, 0:1] - other[:, 0:1]) / COLS
            spread = own[:, 1:2] + other[:, 1:2] + apart * apart * (COLS / 2)
            centre = total / (2 * COLS)
            inv = lax.rsqrt(spread / (2 * COLS) + 1e-06)
            vn[rows, :] = ((act - centre) * inv * v_gain[...]).astype(BF)

        in_rows(i * RB, RB, 64, body)
        low = lax.broadcasted_iota(jnp.int32, (128, 128), 1) < 64
        for pair in range(4):
            lanes = slice(pair * 128, (pair + 1) * 128)
            m = mix[2 * pair : 2 * pair + 2].astype(BF).reshape(256, 128)
            v = jnp.concatenate(
                [vn[i * RB + b * 128 : i * RB + (b + 1) * 128, lanes] for b in range(2)], axis=1
            )
            both = jnp.dot(m, v, preferred_element_type=F32)
            for b in range(2):
                rows = slice(i * RB + b * 128, i * RB + (b + 1) * 128)
                span = slice(b * 128, (b + 1) * 128)
                mixed = jnp.where(low, both[:128, span], both[128:, span]) + bias[:, lanes]
                gated[rows, lanes] = (acc[0, rows, lanes] * mixed).astype(BF)

    def job_out(i):
        chunk(2)
        rows = slice(i * MB, (i + 1) * MB)
        for q in range(4):
            w = gathered_rows(buf, 2, q * 8, 8)
            part[rows, q * COLS : (q + 1) * COLS] = dot_nt(gated[rows, :], w).astype(BF)
        for n in (2 * i, 2 * i + 1):
            block = pl.ds(n * RB, RB)
            exchange(part.at[block], part_in.at[block], 2 + n, f"out{n}")

    def job_mid(i):
        received(f"out{i}")

        def body(rows):
            total = (part[rows, :].astype(F32) + part_in[rows, :].astype(F32)) * scales[0:1, :]
            inv = lax.rsqrt(jnp.sum(total * total, axis=1, keepdims=True) / WIDTH + 1e-06)
            stream = jnp.concatenate(
                [xfull[0, rows, :].astype(F32), xfull[1, rows, :].astype(F32)], axis=1
            )
            value = (stream + total * inv * gain_out[...]).astype(BF)
            xfull[0, rows, :] = value[:, :HALF]
            xfull[1, rows, :] = value[:, HALF:]
            again = value.astype(F32)
            power = jnp.sum(again * again, axis=1, keepdims=True)
            nbuf[rows, :] = (again * lax.rsqrt(power / WIDTH + 1e-06) * gain_up[...]).astype(BF)

        in_rows(i * RB, RB, EB, body, AT_ONCE)

    def job_up(j, i):
        c = 3 + 2 * j
        chunk(c)
        rows = slice(i * MB, (i + 1) * MB)
        raised = jnp.dot(nbuf[rows, :], gathered_rows(buf, c), preferred_element_type=F32)
        raised = jnp.maximum(raised * up_scale[:, j * COLS : (j + 1) * COLS], 0.0)
        vn[rows, :] = (raised * raised).astype(BF)

    def job_dn(j, i):
        c = 4 + 2 * j
        chunk(c)
        rows = slice(i * MB, (i + 1) * MB)
        for q in range(4):
            span = slice((q % 2) * COLS, (q % 2 + 1) * COLS)
            term = dot_nt(vn[rows, :], gathered_rows(buf, c, q * 8, 8))
            acc[q // 2, rows, span] = term if j == 0 else acc[q // 2, rows, span] + term

    def last_down(half, i):
        rows = slice(i * MB, (i + 1) * MB)
        for q in range(2):
            span = slice(q * COLS, (q + 1) * COLS)
            term = dot_nt(vn[rows, :], rows_of_half(buf, NCH - 1, half, q * 8, 8))
            yield rows, span, (acc[half, rows, span] + term).astype(BF)

    def job(name):
        kind, index = name.rstrip("0123456789"), [int(n) for n in name[len(name.rstrip("0123456789")) :]]
        {"xn": job_xn, "u": job_u, "v": job_v, "mix": job_mix, "out": job_out, "mid": job_mid, "up": job_up, "dn": job_dn}[kind](*index)

    send_scales(0)
    turns = {50: 1, 90: 2, 120: 3, 150: 4, 165: 5}
    for n, code in enumerate(PROGRAM):
        if n in turns:
            scales_arrived(turns[n] - 1)
            if turns[n] < STEPS:
                send_scales(turns[n])
            else:
                spread_scales()
        if code >= 220:
            name = JOB_NAMES[code - 220]
            if not name.startswith("dn3"):
                job(name)
        else:
            c, k, r = code // 20, (code // 4) % 5, code % 4
            if k:
                arrived(c, k - 1, r)
            send(c, k, r)

    for i in range(NRB):
        sent(f"out{i}")
    chunk(NCH - 1)
    own, other = lane, 1 - lane
    for i in range(2):
        for rows, span, value in last_down(other, i):
            part[rows, span] = value
        for n in (2 * i, 2 * i + 1):
            block = pl.ds(n * RB, RB)
            exchange(part.at[block, pl.ds(0, HALF)], terms_in.at[block], 6 + n, f"terms{n}")
    for i in range(2):
        for rows, span, value in last_down(own, i):
            acc[own, rows, span] = value.astype(F32)
    own_cols = pl.ds(pl.multiple_of(lane * HALF, HALF), HALF)

    def add_up(rows):
        value = (acc[own, rows, :] + terms_in[rows, :].astype(F32)) * scales[1:2, own_cols]
        acc[own, rows, :] = value
        power = jnp.sum(value * value, axis=1, keepdims=True)
        stats[1, rows, :] = jnp.broadcast_to(power, (EB, 128))

    def finish(rows):
        power = stats[1, rows, 0:1] + stats_in[1, rows, 0:1]
        inv = lax.rsqrt(power / WIDTH + 1e-06)
        value = acc[own, rows, :] * inv * gain_last[:, own_cols]
        result[rows, :] = (xfull[lane, rows, :].astype(F32) + value).astype(BF)

    for i in range(NRB):
        received(f"terms{i}")
        in_rows(i * RB, RB, EB, add_up, AT_ONCE)
        block = pl.ds(i * RB, RB)
        exchange(stats.at[1, block], stats_in.at[1, block], 10 + i, f"power{i}")
    for i in range(NRB):
        received(f"power{i}")
        in_rows(i * RB, RB, EB, finish, AT_ONCE)
    for copy in pending.values():
        copy.wait_send()
    for c in range(NCH):
        block = buf.at[c, :, pl.ds(0, 31)]
        pltpu.make_async_copy(block, block, send_sem.at[c]).wait()
    for k in range(STEPS):
        block = sbuf.at[pl.ds(0, 1 << k)]
        pltpu.make_async_copy(block, block, s_send.at[k]).wait()


def local(
    resid,
    gain_mix_in,
    u_weight,
    v_weight,
    u_scale,
    v_scale,
    v_gain,
    mix_matrix,
    mix_bias,
    out_weight,
    out_scale,
    gain_mix_out,
    gain_ffn_in,
    up_weight,
    up_scale,
    down_weight,
    down_scale,
    gain_ffn_out,
):
    row = lambda a: a.reshape(1, -1)
    vmem = pl.BlockSpec(memory_space=pltpu.VMEM)
    hbm = pl.BlockSpec(memory_space=pl.ANY)
    dma = pltpu.SemaphoreType.DMA
    return pl.pallas_call(
        kernel,
        out_shape=pltpu.VMEM((ROWS, HALF), BF),
        in_specs=[hbm] * 7 + [vmem] * 11,
        out_specs=vmem,
        scratch_shapes=[
            pltpu.VMEM((NCH, PARTS, SHARDS, TILE, COLS), BF),
            pltpu.VMEM((SHARDS, 2, 128), F32),
            pltpu.VMEM((2, WIDTH), F32),
            pltpu.VMEM((8, 128, 128), F32),
            pltpu.VMEM((128, COLS), F32),
            pltpu.VMEM((2, ROWS, HALF), BF),
            pltpu.VMEM((ROWS, WIDTH), BF),
            pltpu.VMEM((2, ROWS, HALF), F32),
            pltpu.VMEM((ROWS, COLS), BF),
            pltpu.VMEM((ROWS, COLS), BF),
            pltpu.VMEM((ROWS, WIDTH), BF),
            pltpu.VMEM((ROWS, WIDTH), BF),
            pltpu.VMEM((ROWS, HALF), BF),
            pltpu.VMEM((2, ROWS, 128), F32),
            pltpu.VMEM((2, ROWS, 128), F32),
            dma((NCH + 1,)),
            dma((NCH,)),
            dma((NCH, STEPS, PARTS)),
            dma((STEPS,)),
            dma((STEPS,)),
            dma((3,)),
            dma((14,)),
            dma((14,)),
        ],
        compiler_params=pltpu.CompilerParams(
            collective_id=0, has_side_effects=True, vmem_limit_bytes=VMEM_LIMIT
        ),
    )(
        u_weight,
        v_weight,
        out_weight.T,
        up_weight,
        down_weight.T,
        resid,
        mix_matrix,
        row(out_scale),
        row(down_scale),
        row(gain_mix_in),
        row(gain_mix_out),
        row(gain_ffn_in),
        row(gain_ffn_out),
        row(u_scale),
        row(v_scale),
        row(v_gain),
        mix_bias,
        row(up_scale),
    )


def solution(mesh):
    in_specs = (
        P(("rep", "fs"), "tp"),
        P(),
        P("fs", "tp"),
        P("fs", "tp"),
        P("tp"),
        P("tp"),
        P("tp"),
        P("tp", None, None),
        P("tp", None),
        P("tp", "fs"),
        P("fs"),
        P(),
        P(),
        P("fs", "tp"),
        P("tp"),
        P("tp", "fs"),
        P("fs"),
        P(),
    )
    out_specs = P(("rep", "fs"), "tp")
    return jax.shard_map(local, mesh=mesh, in_specs=in_specs, out_specs=out_specs, check_vma=False)
```

```python
import itertools

import jax
import jax.numpy as jnp
from jax import lax
from jax.experimental import pallas as pl
from jax.experimental.pallas import tpu as pltpu
from jax.sharding import PartitionSpec as P

MESH = pl.DeviceIdType.MESH
BF = jnp.bfloat16
F32 = jnp.float32

ROWS = 1024
WIDTH = 2048
HALF = 1024
COLS = 512
NCH = 11
LAST = NCH - 1
STEPS = 5
SHARDS = 32
TILE = 16
PARTS = 4
RB = 256
NRB = ROWS // RB
MB = 512
EB = 32
AT_ONCE = 2
VMEM_LIMIT = 58 * 1024 * 1024

CROSSINGS = [
    order
    for z in ("S", "O")
    for order in itertools.permutations(("PX", "QX", "PY", "QY", z))
]
ORDERS = (
    (193, 13, 158, 48),
    (146, 153, 88, 60),
    (6, 180, 124, 209),
    (72, 145, 9, 186),
    (144, 82, 24, 128),
    (87, 156, 64, 72),
    (38, 230, 125, 180),
    (5, 201, 38, 122),
    (24, 191, 128, 188),
    (92, 64, 168, 8),
    (119, 114, 96, 99),
)
SCALE_ORDER = ("PX", "QY", "QX", "PY", "S")
PROGRAM = (
    0, 1, 2, 3, 20, 21, 22, 23, 40, 41, 42, 43, 60, 61, 62, 63, 80, 81, 82, 83,
    100, 101, 102, 103, 121, 122, 123, 140, 141, 120, 143, 161, 163, 200, 201, 202, 180, 162, 142, 181,
    203, 183, 160, 182, 4, 5, 6, 7, 26, 44, 27, 24, 46, 25, 45, 67, 64, 85, 47, 106,
    126, 65, 144, 66, 165, 105, 145, 167, 84, 184, 87, 147, 124, 220, 8, 30, 86, 50, 10, 107,
    127, 221, 9, 31, 28, 104, 89, 130, 222, 11, 29, 49, 51, 125, 110, 166, 223, 69, 70, 148,
    71, 48, 88, 91, 12, 14, 68, 32, 146, 13, 35, 185, 33, 151, 34, 74, 90, 15, 73, 53,
    54, 109, 189, 52, 18, 164, 55, 131, 16, 39, 37, 92, 108, 111, 94, 19, 36, 75, 17, 93,
    58, 38, 59, 56, 57, 72, 77, 129, 128, 95, 224, 186, 187, 149, 112, 114, 96, 225, 150, 76,
    78, 79, 206, 226, 113, 227, 207, 228, 132, 229, 115, 99, 230, 231, 204, 171, 133, 98, 232, 205,
    168, 135, 233, 234, 169, 97, 154, 170, 235, 188, 153, 236, 134, 237, 190, 116, 117, 119, 238, 118,
    239, 191, 155, 240, 152, 241, 208, 209, 242, 210, 211, 172, 175, 136, 139, 243, 173, 138, 244, 137,
    192, 245, 174, 246, 193, 158, 159, 247, 195, 156, 194, 157, 212, 215, 176, 178, 248, 213, 214, 249,
    177, 179, 197, 196, 198, 199, 250, 251, 216, 218, 219, 217, 252, 253, 254, 255, 256, 257,
)
JOB_NAMES = (
    ["xn0", "xn1", "xn2", "xn3", "v0", "v1", "vn0", "vn1", "u0", "mix0", "mix1", "out0"]
    + ["vn2", "vn3", "u1", "mix2", "mix3", "out1", "mid0", "mid1", "up00", "mid2", "mid3", "up01"]
    + ["dn00", "dn01"]
    + [f"{kind}{j}{i}" for j in range(1, 4) for kind in ("up", "dn") for i in range(2)]
)


def link_bits(fs):
    x, y, z = fs % 4, (fs // 4) % 4, fs // 16
    return {
        "PX": (x + x // 2) % 2,
        "QX": x // 2,
        "PY": (y + y // 2) % 2,
        "QY": y // 2,
        "S": z,
        "O": z,
    }


def place(order, fs):
    bits = link_bits(fs)
    return sum(bits[name] * (1 << k) for k, name in enumerate(order))


def order_of(c, r):
    return CROSSINGS[ORDERS[c][r]]


def gathered_rows(buf, c, first=0, count=SHARDS):
    return jnp.concatenate(
        [
            buf[c, r, place(order_of(c, r), s)]
            for s in range(first, first + count)
            for r in range(PARTS)
        ],
        axis=0,
    )


def dot_nt(a, b):
    return lax.dot_general(a, b, (((1,), (1,)), ((), ())), preferred_element_type=F32)


def kernel(
    u_weight,
    v_weight,
    out_weight,
    up_weight,
    down_weight,
    resid,
    mix_matrix,
    out_scale,
    down_scale,
    gain_in,
    gain_out,
    gain_up,
    gain_last,
    u_scale,
    v_scale,
    v_gain,
    mix_bias,
    up_scale,
    result,
    buf,
    sbuf,
    scales,
    mix,
    bias,
    xfull,
    nbuf,
    acc,
    vn,
    both_hid,
    stage,
    gated,
    part,
    part_in,
    terms_in,
    stats,
    stats_in,
    load_sem,
    send_sem,
    recv_sem,
    first_send,
    first_recv,
    s_send,
    s_recv,
    x_sem,
    pair_send,
    pair_recv,
):
    rep, fs, lane = lax.axis_index("rep"), lax.axis_index("fs"), lax.axis_index("tp")
    x, y, z = fs % 4, (fs // 4) % 4, fs // 16
    here = z * 16 + y * 4
    far = (1 - z) * 16 + y * 4 + x
    peer = {
        "PX": (rep, here + x + 1 - 2 * (x % 2), lane),
        "QX": (rep, here + 3 - x, lane),
        "PY": (rep, z * 16 + (y + 1 - 2 * (y % 2)) * 4 + x, lane),
        "QY": (rep, z * 16 + (3 - y) * 4 + x, lane),
        "S": (rep, far, lane),
        "O": (1 - rep, far, lane),
    }
    partner = (rep, fs, 1 - lane)
    across = (rep, far, 1 - lane)
    crossed = lane + z - 2 * lane * z
    used = sorted({order_of(c, r) for c in range(NCH) for r in range(PARTS)} | {SCALE_ORDER})
    places = {order: place(order, fs) for order in used}

    barrier = pltpu.get_barrier_semaphore()
    for device in (*peer.values(), partner, across):
        pl.semaphore_signal(barrier, inc=1, device_id=device, device_id_type=MESH)

    loads = []

    def load(source, first, c, sem):
        slot = acc.at[0, pl.ds(c * 64, 64), pl.ds(0, COLS)]
        copy = pltpu.make_async_copy(source.at[:, pl.ds(first, COLS)], slot, load_sem.at[sem])
        copy.start()
        loads.append(copy)

    for n, source in enumerate((v_weight, u_weight, out_weight)):
        load(source, 0, n, n)
    for j in range(4):
        load(up_weight, j * COLS, 3 + 2 * j, 3 + 2 * j)
        load(down_weight, j * COLS, 4 + 2 * j, 4 + 2 * j)
    own_x = pltpu.make_async_copy(resid, xfull.at[lane], x_sem.at[0])
    own_x.start()
    own_mix = pltpu.make_async_copy(mix_matrix, mix, load_sem.at[NCH])
    own_mix.start()

    for c in range(NCH):
        loads[c].wait()
        for r in range(PARTS):
            value = acc[0, c * 64 + r * TILE : c * 64 + (r + 1) * TILE, :COLS]
            if c < LAST:
                buf[c, r, places[order_of(c, r)]] = value.astype(BF)
            else:
                stage[r] = value.astype(BF)

    def last_slot(r):
        return place(order_of(LAST, r), lane * 16 + y * 4 + x)

    @pl.when(crossed == 0)
    def _():
        for r in range(PARTS):
            buf[LAST, r, last_slot(r)] = stage[r]

    sbuf[places[SCALE_ORDER], 0:1, 0:64] = out_scale[...]
    sbuf[places[SCALE_ORDER], 1:2, 0:64] = down_scale[...]

    pl.semaphore_wait(barrier, 8)

    other_x = pltpu.make_async_remote_copy(
        src_ref=resid,
        dst_ref=xfull.at[lane],
        send_sem=x_sem.at[1],
        recv_sem=x_sem.at[2],
        device_id=partner,
        device_id_type=MESH,
    )
    other_x.start()

    def first_of_last(r):
        slot = buf.at[LAST, r, last_slot(r)]
        pltpu.make_async_remote_copy(
            src_ref=stage.at[r],
            dst_ref=slot,
            send_sem=send_sem.at[LAST],
            recv_sem=first_recv.at[crossed, r],
            device_id=(rep, far, z),
            device_id_type=MESH,
        ).start()

        @pl.when(crossed == 1)
        def _():
            pltpu.make_async_remote_copy(
                src_ref=stage.at[r],
                dst_ref=slot,
                send_sem=first_send.at[r],
                recv_sem=first_recv.at[2, r],
                device_id=partner,
                device_id_type=MESH,
            ).start()

    def first_of_last_arrived(r):
        @pl.when(crossed == 1)
        def _():
            for n in range(2):
                pltpu.make_async_copy(stage.at[r], stage.at[r], first_recv.at[n, r]).wait()

        @pl.when(crossed == 0)
        def _():
            pltpu.make_async_copy(stage.at[r], stage.at[r], first_recv.at[2, r]).wait()

    def send(c, k, r):
        size = 1 << k
        order = order_of(c, r)
        block = buf.at[c, r, pl.ds((places[order] // size) * size, size)]
        pltpu.make_async_remote_copy(
            src_ref=block,
            dst_ref=block,
            send_sem=send_sem.at[c],
            recv_sem=recv_sem.at[c, k, r],
            device_id=peer[order[k]],
            device_id_type=MESH,
        ).start()

    def arrived(c, k, r):
        block = buf.at[c, r, pl.ds(0, 1 << k)]
        pltpu.make_async_copy(block, block, recv_sem.at[c, k, r]).wait()

    complete = set()

    def chunk(c):
        if c not in complete:
            complete.add(c)
            for r in range(PARTS):
                arrived(c, STEPS - 1, r)

    def send_scales(k):
        size = 1 << k
        block = sbuf.at[pl.ds((places[SCALE_ORDER] // size) * size, size)]
        pltpu.make_async_remote_copy(
            src_ref=block,
            dst_ref=block,
            send_sem=s_send.at[k],
            recv_sem=s_recv.at[k],
            device_id=peer[SCALE_ORDER[k]],
            device_id_type=MESH,
        ).start()

    def scales_arrived(k):
        block = sbuf.at[pl.ds(0, 1 << k)]
        pltpu.make_async_copy(block, block, s_recv.at[k]).wait()

    def spread_scales():
        low = lax.broadcasted_iota(jnp.int32, (1, 128), 1) < 64
        for n in range(2):
            for s in range(0, SHARDS, 2):
                a = sbuf[place(SCALE_ORDER, s), n : n + 1, :]
                b = sbuf[place(SCALE_ORDER, s + 1), n : n + 1, :]
                scales[n : n + 1, s * 64 : s * 64 + 128] = jnp.where(low, a, pltpu.roll(b, 64, 1))

    pending, waits, waited = {}, {}, set()

    def exchange(src, dst, index, name):
        copy = pltpu.make_async_remote_copy(
            src_ref=src,
            dst_ref=dst,
            send_sem=pair_send.at[index],
            recv_sem=pair_recv.at[index],
            device_id=partner,
            device_id_type=MESH,
        )
        copy.start()
        pending[name] = copy
        waits[name] = copy

    def received(name):
        if name not in waited:
            waited.add(name)
            waits[name].wait_recv()

    def sent(name):
        pending.pop(name).wait_send()

    def in_rows(first, count, size, body, at_once=1):
        def step(i, carry):
            for n in range(at_once):
                body(pl.ds(pl.multiple_of(first + (i * at_once + n) * size, size), size))
            return carry

        lax.fori_loop(0, count // (size * at_once), step, 0)

    def spread_bias():
        turned = jnp.concatenate([mix_bias[...]] * 16, axis=0).T
        low = lax.broadcasted_iota(jnp.int32, (128, 128), 1) < 64
        for pair in range(4):
            bias[:, pair * 128 : (pair + 1) * 128] = jnp.where(
                low, turned[:, 2 * pair : 2 * pair + 1], turned[:, 2 * pair + 1 : 2 * pair + 2]
            )

    def job_xn(i):
        if i == 0:
            spread_bias()
            own_x.wait()
            other_x.wait()

        def body(rows):
            a = xfull[0, rows, :].astype(F32)
            b = xfull[1, rows, :].astype(F32)
            power = jnp.sum(a * a, axis=1, keepdims=True) + jnp.sum(b * b, axis=1, keepdims=True)
            inv = lax.rsqrt(power / WIDTH + 1e-06)
            nbuf[rows, :HALF] = (a * inv * gain_in[:, :HALF]).astype(BF)
            nbuf[rows, HALF:] = (b * inv * gain_in[:, HALF:]).astype(BF)

        in_rows(i * RB, RB, EB, body, AT_ONCE)

    def job_u(i):
        chunk(1)
        rows = slice(i * MB, (i + 1) * MB)
        pre = jnp.dot(nbuf[rows, :], gathered_rows(buf, 1), preferred_element_type=F32)
        acc[0, rows, :COLS] = jax.nn.gelu(pre * u_scale[...])

    def job_v(i):
        chunk(0)
        rows = slice(i * MB, (i + 1) * MB)
        pre = jnp.dot(nbuf[rows, :], gathered_rows(buf, 0), preferred_element_type=F32)
        act = jax.nn.gelu(pre * v_scale[...])
        acc[0, rows, COLS:] = act
        total = jnp.sum(act, axis=1, keepdims=True)
        off = act - total / COLS
        spread = jnp.sum(off * off, axis=1, keepdims=True)
        lanes = lax.broadcasted_iota(jnp.int32, (MB, 128), 1)
        stats[0, rows, :] = jnp.where(lanes == 0, total, spread)
        exchange(stats.at[0, pl.ds(i * MB, MB)], stats_in.at[0, pl.ds(i * MB, MB)], i, f"v{i}")

    def job_vn(i):
        received(f"v{i // 2}")

        def body(rows):
            act = acc[0, rows, COLS:]
            own, other = stats[0, rows, :], stats_in[0, rows, :]
            total = own[:, 0:1] + other[:, 0:1]
            apart = (own[:, 0:1] - other[:, 0:1]) / COLS
            spread = own[:, 1:2] + other[:, 1:2] + apart * apart * (COLS / 2)
            centre = total / (2 * COLS)
            inv = lax.rsqrt(spread / (2 * COLS) + 1e-06)
            vn[rows, :] = ((act - centre) * inv * v_gain[...]).astype(BF)

        in_rows(i * RB, RB, 64, body)

    def job_mix(i):
        if i == 0:
            own_mix.wait()
        low = lax.broadcasted_iota(jnp.int32, (128, 128), 1) < 64
        for pair in range(4):
            lanes = slice(pair * 128, (pair + 1) * 128)
            m = mix[2 * pair : 2 * pair + 2].astype(BF).reshape(256, 128)
            v = jnp.concatenate(
                [vn[i * RB + b * 128 : i * RB + (b + 1) * 128, lanes] for b in range(2)], axis=1
            )
            both = jnp.dot(m, v, preferred_element_type=F32)
            for b in range(2):
                rows = slice(i * RB + b * 128, i * RB + (b + 1) * 128)
                span = slice(b * 128, (b + 1) * 128)
                mixed = jnp.where(low, both[:128, span], both[128:, span]) + bias[:, lanes]
                gated[rows, lanes] = (acc[0, rows, lanes] * mixed).astype(BF)

    def job_out(i):
        chunk(2)
        rows = slice(i * MB, (i + 1) * MB)
        for q in range(4):
            w = gathered_rows(buf, 2, q * 8, 8)
            part[rows, q * COLS : (q + 1) * COLS] = dot_nt(gated[rows, :], w).astype(BF)
        for n in (2 * i, 2 * i + 1):
            block = pl.ds(n * RB, RB)
            exchange(part.at[block], part_in.at[block], 2 + n, f"out{n}")

    def job_mid(i):
        received(f"out{i}")

        def body(rows):
            total = (part[rows, :].astype(F32) + part_in[rows, :].astype(F32)) * scales[0:1, :]
            inv = lax.rsqrt(jnp.sum(total * total, axis=1, keepdims=True) / WIDTH + 1e-06)
            stream = jnp.concatenate(
                [xfull[0, rows, :].astype(F32), xfull[1, rows, :].astype(F32)], axis=1
            )
            value = (stream + total * inv * gain_out[...]).astype(BF)
            xfull[0, rows, :] = value[:, :HALF]
            xfull[1, rows, :] = value[:, HALF:]
            again = value.astype(F32)
            power = jnp.sum(again * again, axis=1, keepdims=True)
            nbuf[rows, :] = (again * lax.rsqrt(power / WIDTH + 1e-06) * gain_up[...]).astype(BF)

        in_rows(i * RB, RB, EB, body, AT_ONCE)

    def job_up(j, i):
        c = 3 + 2 * j
        chunk(c)
        rows = slice(i * MB, (i + 1) * MB)
        raised = jnp.dot(nbuf[rows, :], gathered_rows(buf, c), preferred_element_type=F32)
        raised = jnp.maximum(raised * up_scale[:, j * COLS : (j + 1) * COLS], 0.0)
        if j < 3:
            vn[rows, :] = (raised * raised).astype(BF)
        else:
            both_hid[lane, rows, :] = (raised * raised).astype(BF)
            block = both_hid.at[lane, pl.ds(i * MB, MB)]
            exchange(block, block, 6 + i, f"hid{i}")

    def job_dn(j, i):
        c = 4 + 2 * j
        chunk(c)
        rows = slice(i * MB, (i + 1) * MB)
        for q in range(4):
            span = slice((q % 2) * COLS, (q % 2 + 1) * COLS)
            term = dot_nt(vn[rows, :], gathered_rows(buf, c, q * 8, 8))
            acc[q // 2, rows, span] = term if j == 0 else acc[q // 2, rows, span] + term
        if j == 2:
            send_terms(i)

    own, other = lane, 1 - lane
    own_cols = pl.ds(pl.multiple_of(lane * HALF, HALF), HALF)

    def send_terms(i):
        for n in (2 * i, 2 * i + 1):
            sent(f"out{n}")

        def body(rows):
            part[rows, :HALF] = acc[other, rows, :].astype(BF)

        in_rows(i * MB, MB, EB, body, AT_ONCE)
        block = pl.ds(i * MB, MB)
        exchange(part.at[block, pl.ds(0, HALF)], terms_in.at[block], 8 + i, f"terms{i}")

    def last_rows(half, first, count):
        return jnp.concatenate(
            [
                buf[LAST, r, place(order_of(LAST, r), half * 16 + s)]
                for s in range(first, first + count)
                for r in range(PARTS)
            ],
            axis=0,
        )

    def last_down(i):
        rows = slice(i * MB, (i + 1) * MB)
        power = None
        for q in range(2):
            span = slice(q * COLS, (q + 1) * COLS)
            scale = scales[1:2, pl.ds(pl.multiple_of(lane * HALF + q * COLS, COLS), COLS)]
            term = dot_nt(both_hid[0, rows, :], last_rows(0, q * 8, 8))
            term = term + dot_nt(both_hid[1, rows, :], last_rows(1, q * 8, 8))
            value = (acc[own, rows, span] + terms_in[rows, span].astype(F32) + term) * scale
            acc[own, rows, span] = value
            square = jnp.sum(value * value, axis=1, keepdims=True)
            power = square if q == 0 else power + square
        stats[1, rows, :] = jnp.broadcast_to(power, (MB, 128))
        block = pl.ds(i * MB, MB)
        exchange(stats.at[1, block], stats_in.at[1, block], 10 + i, f"power{i}")

    def job(name):
        kind, index = name.rstrip("0123456789"), [int(n) for n in name[len(name.rstrip("0123456789")) :]]
        {"xn": job_xn, "u": job_u, "v": job_v, "vn": job_vn, "mix": job_mix, "out": job_out, "mid": job_mid, "up": job_up, "dn": job_dn}[kind](*index)

    send_scales(0)
    turns = {50: 1, 90: 2, 120: 3, 150: 4, 165: 5}
    for n, code in enumerate(PROGRAM):
        if n in turns:
            scales_arrived(turns[n] - 1)
            if turns[n] < STEPS:
                send_scales(turns[n])
            else:
                spread_scales()
        if code >= 220:
            name = JOB_NAMES[code - 220]
            if not name.startswith("dn3"):
                job(name)
        else:
            c, k, r = code // 20, (code // 4) % 5, code % 4
            if c == LAST and k == 0:
                first_of_last(r)
                continue
            if c == LAST and k == 1:
                first_of_last_arrived(r)
            elif k:
                arrived(c, k - 1, r)
            send(c, k, r)

    def finish(rows):
        power = stats[1, rows, 0:1] + stats_in[1, rows, 0:1]
        inv = lax.rsqrt(power / WIDTH + 1e-06)
        value = acc[own, rows, :] * inv * gain_last[:, own_cols]
        result[rows, :] = (xfull[lane, rows, :].astype(F32) + value).astype(BF)

    for i in range(2):
        received(f"hid{i}")
        received(f"terms{i}")
    chunk(LAST)
    for i in range(2):
        last_down(i)
    for i in range(2):
        received(f"power{i}")
        in_rows(i * MB, MB, EB, finish, AT_ONCE)
    for copy in pending.values():
        copy.wait_send()
    for c in range(NCH):
        block = buf.at[c, :, pl.ds(0, 31)]
        pltpu.make_async_copy(block, block, send_sem.at[c]).wait()
    @pl.when(crossed == 1)
    def _():
        for r in range(PARTS):
            pltpu.make_async_copy(stage.at[r], stage.at[r], first_send.at[r]).wait()

    for k in range(STEPS):
        block = sbuf.at[pl.ds(0, 1 << k)]
        pltpu.make_async_copy(block, block, s_send.at[k]).wait()


def local(
    resid,
    gain_mix_in,
    u_weight,
    v_weight,
    u_scale,
    v_scale,
    v_gain,
    mix_matrix,
    mix_bias,
    out_weight,
    out_scale,
    gain_mix_out,
    gain_ffn_in,
    up_weight,
    up_scale,
    down_weight,
    down_scale,
    gain_ffn_out,
):
    row = lambda a: a.reshape(1, -1)
    vmem = pl.BlockSpec(memory_space=pltpu.VMEM)
    hbm = pl.BlockSpec(memory_space=pl.ANY)
    dma = pltpu.SemaphoreType.DMA
    return pl.pallas_call(
        kernel,
        out_shape=pltpu.VMEM((ROWS, HALF), BF),
        in_specs=[hbm] * 7 + [vmem] * 11,
        out_specs=vmem,
        scratch_shapes=[
            pltpu.VMEM((NCH, PARTS, SHARDS, TILE, COLS), BF),
            pltpu.VMEM((SHARDS, 2, 128), F32),
            pltpu.VMEM((2, WIDTH), F32),
            pltpu.VMEM((8, 128, 128), F32),
            pltpu.VMEM((128, COLS), F32),
            pltpu.VMEM((2, ROWS, HALF), BF),
            pltpu.VMEM((ROWS, WIDTH), BF),
            pltpu.VMEM((2, ROWS, HALF), F32),
            pltpu.VMEM((ROWS, COLS), BF),
            pltpu.VMEM((2, ROWS, COLS), BF),
            pltpu.VMEM((PARTS, TILE, COLS), BF),
            pltpu.VMEM((ROWS, COLS), BF),
            pltpu.VMEM((ROWS, WIDTH), BF),
            pltpu.VMEM((ROWS, WIDTH), BF),
            pltpu.VMEM((ROWS, HALF), BF),
            pltpu.VMEM((2, ROWS, 128), F32),
            pltpu.VMEM((2, ROWS, 128), F32),
            dma((NCH + 1,)),
            dma((NCH,)),
            dma((NCH, STEPS, PARTS)),
            dma((PARTS,)),
            dma((3, PARTS)),
            dma((STEPS,)),
            dma((STEPS,)),
            dma((3,)),
            dma((12,)),
            dma((12,)),
        ],
        compiler_params=pltpu.CompilerParams(
            collective_id=0, has_side_effects=True, vmem_limit_bytes=VMEM_LIMIT
        ),
    )(
        u_weight,
        v_weight,
        out_weight.T,
        up_weight,
        down_weight.T,
        resid,
        mix_matrix,
        row(out_scale),
        row(down_scale),
        row(gain_mix_in),
        row(gain_mix_out),
        row(gain_ffn_in),
        row(gain_ffn_out),
        row(u_scale),
        row(v_scale),
        row(v_gain),
        mix_bias,
        row(up_scale),
    )


def solution(mesh):
    in_specs = (
        P(("rep", "fs"), "tp"),
        P(),
        P("fs", "tp"),
        P("fs", "tp"),
        P("tp"),
        P("tp"),
        P("tp"),
        P("tp", None, None),
        P("tp", None),
        P("tp", "fs"),
        P("fs"),
        P(),
        P(),
        P("fs", "tp"),
        P("tp"),
        P("tp", "fs"),
        P("fs"),
        P(),
    )
    out_specs = P(("rep", "fs"), "tp")
    return jax.shard_map(local, mesh=mesh, in_specs=in_specs, out_specs=out_specs, check_vma=False)
```

```python
import itertools

import jax
import jax.numpy as jnp
from jax import lax
from jax.experimental import pallas as pl
from jax.experimental.pallas import tpu as pltpu
from jax.sharding import PartitionSpec as P

MESH = pl.DeviceIdType.MESH
BF = jnp.bfloat16
F32 = jnp.float32

ROWS = 1024
WIDTH = 2048
HALF = 1024
COLS = 512
NCH = 11
LAST = NCH - 1
STEPS = 5
SHARDS = 32
TILE = 16
PARTS = 4
RB = 256
NRB = ROWS // RB
MB = 512
EB = 32
AT_ONCE = 4
VMEM_LIMIT = 58 * 1024 * 1024

CROSSINGS = [
    order
    for z in ("S", "O")
    for order in itertools.permutations(("PX", "QX", "PY", "QY", z))
]
ORDERS = (
    (193, 13, 158, 48),
    (146, 153, 88, 60),
    (6, 180, 124, 209),
    (72, 145, 9, 186),
    (144, 82, 24, 128),
    (87, 156, 64, 72),
    (38, 230, 125, 180),
    (5, 201, 38, 122),
    (24, 191, 128, 188),
    (92, 64, 168, 8),
    (119, 114, 96, 99),
)
SCALE_ORDER = ("PX", "QY", "QX", "PY", "S")
PROGRAM = (
    0, 1, 2, 3, 20, 21, 22, 23, 40, 41, 42, 43, 60, 61, 62, 63, 80, 81, 82, 83,
    100, 101, 102, 103, 121, 122, 123, 140, 141, 120, 143, 161, 163, 200, 201, 202, 180, 162, 142, 181,
    203, 183, 160, 182, 4, 5, 6, 7, 26, 44, 27, 24, 46, 25, 45, 67, 64, 85, 47, 106,
    126, 65, 144, 66, 165, 105, 145, 167, 84, 184, 87, 147, 124, 220, 8, 30, 86, 50, 10, 107,
    127, 221, 9, 31, 28, 104, 89, 130, 222, 11, 29, 49, 51, 125, 110, 166, 223, 69, 70, 148,
    71, 48, 88, 91, 12, 14, 68, 32, 146, 13, 35, 185, 33, 151, 34, 74, 90, 15, 73, 53,
    54, 109, 189, 52, 18, 164, 55, 131, 16, 39, 37, 92, 108, 111, 94, 19, 36, 75, 17, 93,
    58, 38, 59, 56, 57, 72, 77, 129, 128, 95, 224, 186, 187, 149, 112, 114, 96, 225, 150, 76,
    78, 79, 206, 226, 113, 227, 207, 228, 132, 229, 115, 99, 230, 231, 204, 171, 133, 98, 232, 205,
    168, 135, 233, 234, 169, 97, 154, 170, 235, 188, 153, 236, 134, 237, 190, 116, 117, 119, 238, 118,
    239, 191, 155, 240, 152, 241, 208, 209, 242, 210, 211, 172, 175, 136, 139, 243, 173, 138, 244, 137,
    192, 245, 174, 246, 193, 158, 159, 247, 195, 156, 194, 157, 212, 215, 176, 178, 248, 213, 214, 249,
    177, 179, 197, 196, 198, 199, 250, 251, 216, 218, 219, 217, 252, 253, 254, 255, 256, 257,
)
JOB_NAMES = (
    ["xn0", "xn1", "xn2", "xn3", "v0", "v1", "vn0", "vn1", "u0", "mix0", "mix1", "out0"]
    + ["vn2", "vn3", "u1", "mix2", "mix3", "out1", "mid0", "mid1", "up00", "mid2", "mid3", "up01"]
    + ["dn00", "dn01"]
    + [f"{kind}{j}{i}" for j in range(1, 4) for kind in ("up", "dn") for i in range(2)]
)


def link_bits(fs):
    x, y, z = fs % 4, (fs // 4) % 4, fs // 16
    return {
        "PX": (x + x // 2) % 2,
        "QX": x // 2,
        "PY": (y + y // 2) % 2,
        "QY": y // 2,
        "S": z,
        "O": z,
    }


def place(order, fs):
    bits = link_bits(fs)
    return sum(bits[name] * (1 << k) for k, name in enumerate(order))


def order_of(c, r):
    return CROSSINGS[ORDERS[c][r]]


def gathered_rows(buf, c, first=0, count=SHARDS):
    return jnp.concatenate(
        [
            buf[c, r, place(order_of(c, r), s)]
            for s in range(first, first + count)
            for r in range(PARTS)
        ],
        axis=0,
    )


def dot_nt(a, b):
    return lax.dot_general(a, b, (((1,), (1,)), ((), ())), preferred_element_type=F32)


def kernel(
    u_weight,
    v_weight,
    out_weight,
    up_weight,
    down_weight,
    resid,
    mix_matrix,
    out_scale,
    down_scale,
    gain_in,
    gain_out,
    gain_up,
    gain_last,
    u_scale,
    v_scale,
    v_gain,
    mix_bias,
    up_scale,
    result,
    buf,
    sbuf,
    scales,
    mix,
    bias,
    xfull,
    nbuf,
    acc,
    vn,
    both_hid,
    stage,
    gated,
    part,
    part_in,
    terms_in,
    stats,
    stats_in,
    load_sem,
    send_sem,
    recv_sem,
    first_send,
    first_recv,
    s_send,
    s_recv,
    x_sem,
    pair_send,
    pair_recv,
):
    rep, fs, lane = lax.axis_index("rep"), lax.axis_index("fs"), lax.axis_index("tp")
    x, y, z = fs % 4, (fs // 4) % 4, fs // 16
    here = z * 16 + y * 4
    far = (1 - z) * 16 + y * 4 + x
    peer = {
        "PX": (rep, here + x + 1 - 2 * (x % 2), lane),
        "QX": (rep, here + 3 - x, lane),
        "PY": (rep, z * 16 + (y + 1 - 2 * (y % 2)) * 4 + x, lane),
        "QY": (rep, z * 16 + (3 - y) * 4 + x, lane),
        "S": (rep, far, lane),
        "O": (1 - rep, far, lane),
    }
    partner = (rep, fs, 1 - lane)
    across = (rep, far, 1 - lane)
    crossed = lane + z - 2 * lane * z
    used = sorted({order_of(c, r) for c in range(NCH) for r in range(PARTS)} | {SCALE_ORDER})
    places = {order: place(order, fs) for order in used}

    barrier = pltpu.get_barrier_semaphore()
    for device in (*peer.values(), partner, across):
        pl.semaphore_signal(barrier, inc=1, device_id=device, device_id_type=MESH)

    loads = []

    def load(source, first, c, sem):
        slot = acc.at[0, pl.ds(c * 64, 64), pl.ds(0, COLS)]
        copy = pltpu.make_async_copy(source.at[:, pl.ds(first, COLS)], slot, load_sem.at[sem])
        copy.start()
        loads.append(copy)

    for n, source in enumerate((v_weight, u_weight, out_weight)):
        load(source, 0, n, n)
    for j in range(4):
        load(up_weight, j * COLS, 3 + 2 * j, 3 + 2 * j)
        load(down_weight, j * COLS, 4 + 2 * j, 4 + 2 * j)
    own_x = pltpu.make_async_copy(resid, xfull.at[lane], x_sem.at[0])
    own_x.start()
    own_mix = pltpu.make_async_copy(mix_matrix, mix, load_sem.at[NCH])
    own_mix.start()

    for c in range(NCH):
        loads[c].wait()
        for r in range(PARTS):
            value = acc[0, c * 64 + r * TILE : c * 64 + (r + 1) * TILE, :COLS]
            if c < LAST:
                buf[c, r, places[order_of(c, r)]] = value.astype(BF)
            else:
                stage[r] = value.astype(BF)

    def last_slot(r):
        return place(order_of(LAST, r), lane * 16 + y * 4 + x)

    @pl.when(crossed == 0)
    def _():
        for r in range(PARTS):
            buf[LAST, r, last_slot(r)] = stage[r]

    sbuf[places[SCALE_ORDER], 0:1, 0:64] = out_scale[...]
    sbuf[places[SCALE_ORDER], 1:2, 0:64] = down_scale[...]

    pl.semaphore_wait(barrier, 8)

    other_x = pltpu.make_async_remote_copy(
        src_ref=resid,
        dst_ref=xfull.at[lane],
        send_sem=x_sem.at[1],
        recv_sem=x_sem.at[2],
        device_id=partner,
        device_id_type=MESH,
    )
    other_x.start()

    def first_of_last(r):
        slot = buf.at[LAST, r, last_slot(r)]
        pltpu.make_async_remote_copy(
            src_ref=stage.at[r],
            dst_ref=slot,
            send_sem=send_sem.at[LAST],
            recv_sem=first_recv.at[crossed, r],
            device_id=(rep, far, z),
            device_id_type=MESH,
        ).start()

        @pl.when(crossed == 1)
        def _():
            pltpu.make_async_remote_copy(
                src_ref=stage.at[r],
                dst_ref=slot,
                send_sem=first_send.at[r],
                recv_sem=first_recv.at[2, r],
                device_id=partner,
                device_id_type=MESH,
            ).start()

    def first_of_last_arrived(r):
        @pl.when(crossed == 1)
        def _():
            for n in range(2):
                pltpu.make_async_copy(stage.at[r], stage.at[r], first_recv.at[n, r]).wait()

        @pl.when(crossed == 0)
        def _():
            pltpu.make_async_copy(stage.at[r], stage.at[r], first_recv.at[2, r]).wait()

    def send(c, k, r):
        size = 1 << k
        order = order_of(c, r)
        block = buf.at[c, r, pl.ds((places[order] // size) * size, size)]
        pltpu.make_async_remote_copy(
            src_ref=block,
            dst_ref=block,
            send_sem=send_sem.at[c],
            recv_sem=recv_sem.at[c, k, r],
            device_id=peer[order[k]],
            device_id_type=MESH,
        ).start()

    def arrived(c, k, r):
        block = buf.at[c, r, pl.ds(0, 1 << k)]
        pltpu.make_async_copy(block, block, recv_sem.at[c, k, r]).wait()

    complete = set()

    def chunk(c):
        if c not in complete:
            complete.add(c)
            for r in range(PARTS):
                arrived(c, STEPS - 1, r)

    def send_scales(k):
        size = 1 << k
        block = sbuf.at[pl.ds((places[SCALE_ORDER] // size) * size, size)]
        pltpu.make_async_remote_copy(
            src_ref=block,
            dst_ref=block,
            send_sem=s_send.at[k],
            recv_sem=s_recv.at[k],
            device_id=peer[SCALE_ORDER[k]],
            device_id_type=MESH,
        ).start()

    def scales_arrived(k):
        block = sbuf.at[pl.ds(0, 1 << k)]
        pltpu.make_async_copy(block, block, s_recv.at[k]).wait()

    def spread_scales():
        low = lax.broadcasted_iota(jnp.int32, (1, 128), 1) < 64
        for n in range(2):
            for s in range(0, SHARDS, 2):
                a = sbuf[place(SCALE_ORDER, s), n : n + 1, :]
                b = sbuf[place(SCALE_ORDER, s + 1), n : n + 1, :]
                scales[n : n + 1, s * 64 : s * 64 + 128] = jnp.where(low, a, pltpu.roll(b, 64, 1))

    pending, waits, waited = {}, {}, set()

    def exchange(src, dst, index, name):
        copy = pltpu.make_async_remote_copy(
            src_ref=src,
            dst_ref=dst,
            send_sem=pair_send.at[index],
            recv_sem=pair_recv.at[index],
            device_id=partner,
            device_id_type=MESH,
        )
        copy.start()
        pending[name] = copy
        waits[name] = copy

    def received(name):
        if name not in waited:
            waited.add(name)
            waits[name].wait_recv()

    def sent(name):
        pending.pop(name).wait_send()

    def in_rows(first, count, size, body, at_once=1):
        def step(i, carry):
            for n in range(at_once):
                body(pl.ds(pl.multiple_of(first + (i * at_once + n) * size, size), size))
            return carry

        lax.fori_loop(0, count // (size * at_once), step, 0)

    def spread_bias():
        turned = jnp.concatenate([mix_bias[...]] * 16, axis=0).T
        low = lax.broadcasted_iota(jnp.int32, (128, 128), 1) < 64
        for pair in range(4):
            bias[:, pair * 128 : (pair + 1) * 128] = jnp.where(
                low, turned[:, 2 * pair : 2 * pair + 1], turned[:, 2 * pair + 1 : 2 * pair + 2]
            )

    def job_xn(i):
        if i == 0:
            spread_bias()
            own_x.wait()
            other_x.wait()

        def body(rows):
            a = xfull[0, rows, :].astype(F32)
            b = xfull[1, rows, :].astype(F32)
            power = jnp.sum(a * a, axis=1, keepdims=True) + jnp.sum(b * b, axis=1, keepdims=True)
            inv = lax.rsqrt(power / WIDTH + 1e-06)
            nbuf[rows, :HALF] = (a * inv * gain_in[:, :HALF]).astype(BF)
            nbuf[rows, HALF:] = (b * inv * gain_in[:, HALF:]).astype(BF)

        in_rows(i * RB, RB, EB, body, AT_ONCE)

    def job_u(i):
        chunk(1)
        rows = slice(i * MB, (i + 1) * MB)
        pre = jnp.dot(nbuf[rows, :], gathered_rows(buf, 1), preferred_element_type=F32)
        acc[0, rows, :COLS] = jax.nn.gelu(pre * u_scale[...])

    def job_v(i):
        chunk(0)
        rows = slice(i * MB, (i + 1) * MB)
        pre = jnp.dot(nbuf[rows, :], gathered_rows(buf, 0), preferred_element_type=F32)
        act = jax.nn.gelu(pre * v_scale[...])
        acc[0, rows, COLS:] = act
        total = jnp.sum(act, axis=1, keepdims=True)
        off = act - total / COLS
        spread = jnp.sum(off * off, axis=1, keepdims=True)
        lanes = lax.broadcasted_iota(jnp.int32, (MB, 128), 1)
        stats[0, rows, :] = jnp.where(lanes == 0, total, spread)
        exchange(stats.at[0, pl.ds(i * MB, MB)], stats_in.at[0, pl.ds(i * MB, MB)], i, f"v{i}")

    def job_vn(i):
        received(f"v{i // 2}")

        def body(rows):
            act = acc[0, rows, COLS:]
            own, other = stats[0, rows, :], stats_in[0, rows, :]
            total = own[:, 0:1] + other[:, 0:1]
            apart = (own[:, 0:1] - other[:, 0:1]) / COLS
            spread = own[:, 1:2] + other[:, 1:2] + apart * apart * (COLS / 2)
            centre = total / (2 * COLS)
            inv = lax.rsqrt(spread / (2 * COLS) + 1e-06)
            vn[rows, :] = ((act - centre) * inv * v_gain[...]).astype(BF)

        in_rows(i * RB, RB, 64, body)

    def job_mix(i):
        if i == 0:
            own_mix.wait()
        low = lax.broadcasted_iota(jnp.int32, (128, 128), 1) < 64
        for pair in range(4):
            lanes = slice(pair * 128, (pair + 1) * 128)
            m = mix[2 * pair : 2 * pair + 2].astype(BF).reshape(256, 128)
            v = jnp.concatenate(
                [vn[i * RB + b * 128 : i * RB + (b + 1) * 128, lanes] for b in range(2)], axis=1
            )
            both = jnp.dot(m, v, preferred_element_type=F32)
            for b in range(2):
                rows = slice(i * RB + b * 128, i * RB + (b + 1) * 128)
                span = slice(b * 128, (b + 1) * 128)
                mixed = jnp.where(low, both[:128, span], both[128:, span]) + bias[:, lanes]
                gated[rows, lanes] = (acc[0, rows, lanes] * mixed).astype(BF)

    def job_out(i):
        chunk(2)
        rows = slice(i * MB, (i + 1) * MB)
        for q in range(4):
            w = gathered_rows(buf, 2, q * 8, 8)
            part[rows, q * COLS : (q + 1) * COLS] = dot_nt(gated[rows, :], w).astype(BF)
        for n in (2 * i, 2 * i + 1):
            block = pl.ds(n * RB, RB)
            exchange(part.at[block], part_in.at[block], 2 + n, f"out{n}")

    def job_mid(i):
        received(f"out{i}")

        def body(rows):
            total = (part[rows, :].astype(F32) + part_in[rows, :].astype(F32)) * scales[0:1, :]
            inv = lax.rsqrt(jnp.sum(total * total, axis=1, keepdims=True) / WIDTH + 1e-06)
            stream = jnp.concatenate(
                [xfull[0, rows, :].astype(F32), xfull[1, rows, :].astype(F32)], axis=1
            )
            value = (stream + total * inv * gain_out[...]).astype(BF)
            xfull[0, rows, :] = value[:, :HALF]
            xfull[1, rows, :] = value[:, HALF:]
            again = value.astype(F32)
            power = jnp.sum(again * again, axis=1, keepdims=True)
            nbuf[rows, :] = (again * lax.rsqrt(power / WIDTH + 1e-06) * gain_up[...]).astype(BF)

        in_rows(i * RB, RB, EB, body, AT_ONCE)

    def job_up(j, i):
        c = 3 + 2 * j
        chunk(c)
        rows = slice(i * MB, (i + 1) * MB)
        raised = jnp.dot(nbuf[rows, :], gathered_rows(buf, c), preferred_element_type=F32)
        raised = jnp.maximum(raised * up_scale[:, j * COLS : (j + 1) * COLS], 0.0)
        if j < 3:
            vn[rows, :] = (raised * raised).astype(BF)
        else:
            both_hid[lane, rows, :] = (raised * raised).astype(BF)
            block = both_hid.at[lane, pl.ds(i * MB, MB)]
            exchange(block, block, 6 + i, f"hid{i}")

    def job_dn(j, i):
        c = 4 + 2 * j
        chunk(c)
        rows = slice(i * MB, (i + 1) * MB)
        for q in range(4):
            span = slice((q % 2) * COLS, (q % 2 + 1) * COLS)
            term = dot_nt(vn[rows, :], gathered_rows(buf, c, q * 8, 8))
            acc[q // 2, rows, span] = term if j == 0 else acc[q // 2, rows, span] + term
        if j == 2:
            send_terms(i)

    own, other = lane, 1 - lane
    own_cols = pl.ds(pl.multiple_of(lane * HALF, HALF), HALF)

    def send_terms(i):
        for n in (2 * i, 2 * i + 1):
            sent(f"out{n}")

        def body(rows):
            part[rows, :HALF] = acc[other, rows, :].astype(BF)

        in_rows(i * MB, MB, EB, body, AT_ONCE)
        block = pl.ds(i * MB, MB)
        exchange(part.at[block, pl.ds(0, HALF)], terms_in.at[block], 8 + i, f"terms{i}")

    def last_rows(half, first, count):
        return jnp.concatenate(
            [
                buf[LAST, r, place(order_of(LAST, r), half * 16 + s)]
                for s in range(first, first + count)
                for r in range(PARTS)
            ],
            axis=0,
        )

    def last_down(i):
        rows = slice(i * MB, (i + 1) * MB)
        power = None
        for q in range(2):
            span = slice(q * COLS, (q + 1) * COLS)
            scale = scales[1:2, pl.ds(pl.multiple_of(lane * HALF + q * COLS, COLS), COLS)]
            term = dot_nt(both_hid[0, rows, :], last_rows(0, q * 8, 8))
            term = term + dot_nt(both_hid[1, rows, :], last_rows(1, q * 8, 8))
            value = (acc[own, rows, span] + terms_in[rows, span].astype(F32) + term) * scale
            acc[own, rows, span] = value
            square = jnp.sum(value * value, axis=1, keepdims=True)
            power = square if q == 0 else power + square
        stats[1, rows, :] = jnp.broadcast_to(power, (MB, 128))
        block = pl.ds(i * MB, MB)
        exchange(stats.at[1, block], stats_in.at[1, block], 10 + i, f"power{i}")

    def job(name):
        kind, index = name.rstrip("0123456789"), [int(n) for n in name[len(name.rstrip("0123456789")) :]]
        {"xn": job_xn, "u": job_u, "v": job_v, "vn": job_vn, "mix": job_mix, "out": job_out, "mid": job_mid, "up": job_up, "dn": job_dn}[kind](*index)

    send_scales(0)
    turns = {50: 1, 90: 2, 120: 3, 150: 4, 165: 5}
    for n, code in enumerate(PROGRAM):
        if n in turns:
            scales_arrived(turns[n] - 1)
            if turns[n] < STEPS:
                send_scales(turns[n])
            else:
                spread_scales()
        if code >= 220:
            name = JOB_NAMES[code - 220]
            if not name.startswith("dn3"):
                job(name)
        else:
            c, k, r = code // 20, (code // 4) % 5, code % 4
            if c == LAST and k == 0:
                first_of_last(r)
                continue
            if c == LAST and k == 1:
                first_of_last_arrived(r)
            elif k:
                arrived(c, k - 1, r)
            send(c, k, r)

    def finish(rows):
        power = stats[1, rows, 0:1] + stats_in[1, rows, 0:1]
        inv = lax.rsqrt(power / WIDTH + 1e-06)
        value = acc[own, rows, :] * inv * gain_last[:, own_cols]
        result[rows, :] = (xfull[lane, rows, :].astype(F32) + value).astype(BF)

    for i in range(2):
        received(f"hid{i}")
        received(f"terms{i}")
    chunk(LAST)
    for i in range(2):
        last_down(i)
    for i in range(2):
        received(f"power{i}")
        in_rows(i * MB, MB, EB, finish, AT_ONCE)
    for copy in pending.values():
        copy.wait_send()
    for c in range(NCH):
        block = buf.at[c, :, pl.ds(0, 31)]
        pltpu.make_async_copy(block, block, send_sem.at[c]).wait()
    @pl.when(crossed == 1)
    def _():
        for r in range(PARTS):
            pltpu.make_async_copy(stage.at[r], stage.at[r], first_send.at[r]).wait()

    for k in range(STEPS):
        block = sbuf.at[pl.ds(0, 1 << k)]
        pltpu.make_async_copy(block, block, s_send.at[k]).wait()


def local(
    resid,
    gain_mix_in,
    u_weight,
    v_weight,
    u_scale,
    v_scale,
    v_gain,
    mix_matrix,
    mix_bias,
    out_weight,
    out_scale,
    gain_mix_out,
    gain_ffn_in,
    up_weight,
    up_scale,
    down_weight,
    down_scale,
    gain_ffn_out,
):
    row = lambda a: a.reshape(1, -1)
    vmem = pl.BlockSpec(memory_space=pltpu.VMEM)
    hbm = pl.BlockSpec(memory_space=pl.ANY)
    dma = pltpu.SemaphoreType.DMA
    return pl.pallas_call(
        kernel,
        out_shape=pltpu.VMEM((ROWS, HALF), BF),
        in_specs=[hbm] * 7 + [vmem] * 11,
        out_specs=vmem,
        scratch_shapes=[
            pltpu.VMEM((NCH, PARTS, SHARDS, TILE, COLS), BF),
            pltpu.VMEM((SHARDS, 2, 128), F32),
            pltpu.VMEM((2, WIDTH), F32),
            pltpu.VMEM((8, 128, 128), F32),
            pltpu.VMEM((128, COLS), F32),
            pltpu.VMEM((2, ROWS, HALF), BF),
            pltpu.VMEM((ROWS, WIDTH), BF),
            pltpu.VMEM((2, ROWS, HALF), F32),
            pltpu.VMEM((ROWS, COLS), BF),
            pltpu.VMEM((2, ROWS, COLS), BF),
            pltpu.VMEM((PARTS, TILE, COLS), BF),
            pltpu.VMEM((ROWS, COLS), BF),
            pltpu.VMEM((ROWS, WIDTH), BF),
            pltpu.VMEM((ROWS, WIDTH), BF),
            pltpu.VMEM((ROWS, HALF), BF),
            pltpu.VMEM((2, ROWS, 128), F32),
            pltpu.VMEM((2, ROWS, 128), F32),
            dma((NCH + 1,)),
            dma((NCH,)),
            dma((NCH, STEPS, PARTS)),
            dma((PARTS,)),
            dma((3, PARTS)),
            dma((STEPS,)),
            dma((STEPS,)),
            dma((3,)),
            dma((12,)),
            dma((12,)),
        ],
        compiler_params=pltpu.CompilerParams(
            collective_id=0, has_side_effects=True, vmem_limit_bytes=VMEM_LIMIT
        ),
    )(
        u_weight,
        v_weight,
        out_weight.T,
        up_weight,
        down_weight.T,
        resid,
        mix_matrix,
        row(out_scale),
        row(down_scale),
        row(gain_mix_in),
        row(gain_mix_out),
        row(gain_ffn_in),
        row(gain_ffn_out),
        row(u_scale),
        row(v_scale),
        row(v_gain),
        mix_bias,
        row(up_scale),
    )


def solution(mesh):
    in_specs = (
        P(("rep", "fs"), "tp"),
        P(),
        P("fs", "tp"),
        P("fs", "tp"),
        P("tp"),
        P("tp"),
        P("tp"),
        P("tp", None, None),
        P("tp", None),
        P("tp", "fs"),
        P("fs"),
        P(),
        P(),
        P("fs", "tp"),
        P("tp"),
        P("tp", "fs"),
        P("fs"),
        P(),
    )
    out_specs = P(("rep", "fs"), "tp")
    return jax.shard_map(local, mesh=mesh, in_specs=in_specs, out_specs=out_specs, check_vma=False)
```
